256 devices in a mesh: grp: 4 (over y, x), ep: 32 (over z), tp: 2 (over core).
Axes of the slice: x: 2, y: 2, z: 32, core: 2. Of those that a mesh axis runs over, the one named last changes fastest.
The devices are a block of a 4x8x32 slice.
Arguments:
- tokens: bfloat16 [8192, 2048], P(('grp', 'ep')), parts along dimension 0, may hold values from -6 to 6
- norm_gain: float32 [2048], replicated, may hold values from 0.1 to 1.9
- groups: int32 [8192], P(('grp', 'ep')), parts along dimension 0, may hold values from 0 to 1, as said below
- picks: int32 [8192, 4], P(('grp', 'ep')), parts along dimension 0, may hold values from 0 to 31, as said below
- gates: float32 [8192, 4], P(('grp', 'ep')), parts along dimension 0, may hold values from 0.1 to 1
- w_gate: bfloat16 [64, 2048, 512], P('ep', None, 'tp'), may hold values from -0.125 to 0.125
- w_up: bfloat16 [64, 2048, 512], P('ep', None, 'tp'), may hold values from -0.125 to 0.125
- w_down: bfloat16 [64, 512, 2048], P('ep', 'tp'), may hold values from -0.25 to 0.25
Outputs:
- mixed: bfloat16 [8192, 2048], P(('grp', 'ep'), 'tp'), parts along dimension 0
The draws below stay inside these ranges and needn't reach their ends.
There are 4 independent parts, one for each index of `grp`. The reference program is written for one: setup_inputs(seed, part) draws one part's arguments, and reference() takes and returns one part's arrays. A program takes and returns all parts, laid end to end along the dimension named above; an argument that names none is the same for every part. Nothing has to cross between parts.
Inputs may be any that keep to these rules, and one draw needn't show every extreme that they name: `groups`: among the tokens of one device, exactly 8 lie in one common group and all of them name one common expert of it as their first pick; every other token of that device lies in another group. A token's 4 picks are distinct. Among the tokens of one device at most 8 name any one expert (group and pick together), and in every draw one expert is named by exactly 8 tokens of every device.
All inputs are finite; a program needn't handle non-finite values.
Results may differ from the reference program's by a relative error of at most 0.014.
Values may be sent and summed in bfloat16 or wider, within the bound.
A program may use at most 64 MiB of HBM per device.

```python
import math
import jax
import jax.numpy as jnp
from jax import lax

D = 2048
FFE = 512
GROUPS = 2
TOP_K = 4
TOK_DEV = 64
EXPERTS = 64
GROUP_EXPERTS = 32
CAP = 8
TOKENS = 2048
N_EP = 32
N_TP = 2


def routing_tables(key):
    base = jax.random.fold_in(key, 7)
    keys = jax.random.split(base, 3)
    hot_group = jax.random.randint(keys[0], (), 0, GROUPS)
    hot_expert = jax.random.randint(keys[1], (), 0, GROUP_EXPERTS)
    slot = jnp.arange(TOP_K, dtype=jnp.int32)

    def one_block(block_key):
        key_perm, key_hot, key_rest, key_group = jax.random.split(block_key, 4)
        order = jax.random.permutation(key_perm, TOK_DEV).astype(jnp.int32)
        offset_hot = jax.random.randint(key_hot, (), 0, GROUP_EXPERTS - 1)
        offset_rest = jax.random.randint(key_rest, (), 0, GROUP_EXPERTS)
        other = (hot_group + 1 + jax.random.randint(key_group, (TOK_DEV,), 0, GROUPS - 1)) % GROUPS
        is_hot = order < CAP
        step_hot = order[:, None] * (TOP_K - 1) + slot[None, :] - 1
        hot_values = jnp.where(slot[None, :] == 0, hot_expert, (hot_expert + 1 + (offset_hot + step_hot) % (GROUP_EXPERTS - 1)) % GROUP_EXPERTS)
        step_rest = (order[:, None] - CAP) * TOP_K + slot[None, :]
        rest_values = (offset_rest + step_rest) % GROUP_EXPERTS
        chosen = jnp.where(is_hot[:, None], hot_values, rest_values)
        group_of = jnp.where(is_hot, hot_group, other)
        return (group_of.astype(jnp.int32), chosen.astype(jnp.int32))
    block_keys = jax.random.split(keys[2], TOKENS // TOK_DEV)
    group_of, chosen = jax.vmap(one_block)(block_keys)
    return (group_of.reshape(TOKENS), chosen.reshape(TOKENS, TOP_K))


def draw_groups(key, part):
    return routing_tables(key)[0]


def draw_picks(key, part):
    return routing_tables(key)[1]


def block_scale(rng, shape, cuts, low, high):
    factor_of, own = 1.0, jax.random.fold_in(rng, 6)
    for dim, blocks in cuts:
        steps = jnp.exp(jax.random.uniform(jax.random.fold_in(own, dim), (blocks,), jnp.float32, low / len(cuts), high / len(cuts)))
        factor_of = factor_of * jnp.repeat(steps, shape[dim] // blocks).reshape([-1 if axis == dim else 1 for axis in range(len(shape))])
    return factor_of


def bell_draw(own_key, dims, scale, bound, shards=(), kind=jnp.bfloat16):
    result = scale * jax.random.normal(own_key, dims, jnp.float32)
    if shards:
        result = result * block_scale(own_key, dims, shards, -0.22, 0.18)
    return jnp.clip(result, -bound, bound).astype(kind)


def setup_inputs(seed: int = 0, part: int = 0) -> dict:
    key_list = jax.random.split(jax.random.key(seed), 9)
    own_keys = jax.random.split(jax.random.fold_in(key_list[8], part), 9)
    tokens = bell_draw(own_keys[0], (TOKENS, D), 1.0, 6.0, ((0, 32),))
    norm_gain = jnp.clip(1.0 + 0.18 * jax.random.normal(key_list[1], (D,), jnp.float32), 0.1, 1.9)
    groups = draw_groups(jax.random.fold_in(jax.random.fold_in(key_list[8], part), 71), part)
    picks = draw_picks(jax.random.fold_in(jax.random.fold_in(key_list[8], part), 71), part)
    gates = jnp.clip(jnp.exp(math.log(1.0) - 2.3025851 * jax.random.uniform(own_keys[4], (TOKENS, TOP_K), jnp.float32) ** block_scale(own_keys[4], (TOKENS, TOP_K), ((0, 32),), -0.2, 0.2)), 0.1, 1.0)
    w_gate = bell_draw(key_list[5], (EXPERTS, D, FFE), D ** -0.5, 0.125, ((0, 32), (2, 2)))
    w_up = bell_draw(key_list[6], (EXPERTS, D, FFE), D ** -0.5, 0.125, ((0, 32), (2, 2)))
    w_down = bell_draw(key_list[7], (EXPERTS, FFE, D), FFE ** -0.5, 0.25, ((0, 32), (1, 2)))
    return dict(tokens=tokens, norm_gain=norm_gain, groups=groups, picks=picks, gates=gates, w_gate=w_gate, w_up=w_up, w_down=w_down)


epsilon = 1e-06

def reference(tokens, norm_gain, groups, picks, gates, w_gate, w_up, w_down):
    values = tokens.astype(jnp.float32)
    normed = (values * lax.rsqrt(lax.optimization_barrier(jnp.mean(values * values, axis=-1, keepdims=True)) + epsilon) * norm_gain.astype(jnp.float32)).astype(jnp.bfloat16)
    expert_id = groups[:, None] * GROUP_EXPERTS + picks
    limit = N_EP * CAP
    slots = jnp.arange(limit, dtype=jnp.int32)

    def per_expert(total, inputs):
        expert, wg, wu, wd = inputs
        hit = expert_id == expert
        gate_me = lax.optimization_barrier(jnp.sum(jnp.where(hit, gates, 0.0), axis=1))
        present = jnp.any(hit, axis=1)
        position = jnp.cumsum(present.astype(jnp.int32)) - 1
        select = jnp.logical_and(position[None, :] == slots[:, None], present[None, :]).astype(jnp.float32)
        rows = jnp.dot(select.astype(jnp.bfloat16), normed, preferred_element_type=jnp.float32).astype(jnp.bfloat16)
        gate_pre = jnp.dot(rows, wg, preferred_element_type=jnp.float32)
        up_pre = jnp.dot(rows, wu, preferred_element_type=jnp.float32)
        hidden = (jax.nn.silu(gate_pre) * up_pre).astype(jnp.bfloat16)
        blocks = hidden.reshape(limit, N_TP, FFE // N_TP).astype(jnp.float32)
        down = wd.reshape(N_TP, FFE // N_TP, D).astype(jnp.float32)
        parts = jnp.einsum('rkf,kfd->krd', blocks, down).astype(jnp.bfloat16)
        expert_out = lax.optimization_barrier(jnp.sum(parts.astype(jnp.float32), axis=0)).astype(jnp.bfloat16)
        weighted = (select * gate_me[None, :]).T
        return (total + jnp.dot(weighted, expert_out.astype(jnp.float32), precision=lax.Precision.HIGHEST), None)
    start = jnp.zeros((tokens.shape[0], D), jnp.float32)
    total, unused = lax.scan(per_expert, start, (jnp.arange(EXPERTS, dtype=jnp.int32), w_gate, w_up, w_down))
    return total.astype(jnp.bfloat16)
```

```python
import functools

import jax
import jax.numpy as jnp
from jax import lax
from jax.experimental import pallas as pl
from jax.experimental.pallas import tpu as pltpu
from jax.sharding import PartitionSpec as P

GROUPS = 2
MESH = pl.DeviceIdType.MESH
F32 = jnp.float32
BF16 = jnp.bfloat16
CW = 256
META = 16
BATCH = 4

epsilon = 1e-06


def dot(a, b):
    return jnp.dot(a, b, preferred_element_type=F32)


def kernel(
    n, rows, width, local, cap, ffl,
    tok_ref, gain_ref, meta_ref, wg_hbm, wu_hbm, wd_hbm, out_ref,
    own, ag, rs, rs0, contrib, wg, wu, wd, x_own, x_sib, p_own, p_sib, p_rcv, fin,
    sel, gsel, meta_s, rank_s, upper, hid,
    ag_ss, ag_rs, rs_ss, rs_rs, x_ss, x_rs, p_ss, p_rs, f_ss, f_rs, w_sem, own_sem,
):
    slots = n // 2
    batches = slots // BATCH
    nch = width // CW
    half_ch = nch // 2
    me = lax.axis_index("ep")
    tp = lax.axis_index("tp")
    right, left = lax.rem(me + 1, n), lax.rem(me + n - 1, n)
    ahead = jnp.where(tp == 1, right, left)
    behind = jnp.where(tp == 1, left, right)
    reach = slots - 1 + tp
    sibling = 1 - tp

    barrier = pltpu.get_barrier_semaphore()
    pl.semaphore_signal(barrier, inc=1, device_id={"ep": right}, device_id_type=MESH)
    pl.semaphore_signal(barrier, inc=1, device_id={"ep": left}, device_id_type=MESH)
    pl.semaphore_signal(barrier, inc=1, device_id={"tp": sibling}, device_id_type=MESH)

    w_copies = [
        pltpu.make_async_copy(src, dst, w_sem.at[i])
        for i, (src, dst) in enumerate(((wg_hbm, wg), (wu_hbm, wu), (wd_hbm, wd)))
    ]
    for copy in w_copies:
        copy.start()

    m = meta_ref[...]
    hi = m.astype(BF16).astype(F32)
    mid = (m - hi).astype(BF16).astype(F32)
    low = m - hi - mid
    row16 = lax.broadcasted_iota(jnp.int32, m.shape, 0)
    own[0:META, :] = jnp.where(row16 < 8, hi, jnp.where(row16 < 12, mid, low)).astype(BF16)

    total = jnp.zeros((rows, 1), F32)
    for c in range(nch):
        v = tok_ref[:, c * CW:(c + 1) * CW].astype(F32)
        total = total + jnp.sum(v * v, axis=1, keepdims=True)
    scale = lax.rsqrt(total / width + epsilon)
    for c in range(nch):
        v = tok_ref[:, c * CW:(c + 1) * CW].astype(F32)
        own[META + rows * c:META + rows * (c + 1), :] = (
            v * scale * gain_ref[:, c * CW:(c + 1) * CW]
        ).astype(BF16)

    ri = lax.broadcasted_iota(jnp.int32, (BATCH * rows, BATCH * rows), 0)
    ci = lax.broadcasted_iota(jnp.int32, (BATCH * rows, BATCH * rows), 1)
    upper[...] = jnp.where((ri // rows == ci // rows) & (ri < ci), 1.0, 0.0).astype(BF16)

    own_copy = pltpu.make_async_copy(own, ag.at[slots - 1], own_sem)

    @pl.when(tp == 0)
    def _():
        own_copy.start()

    pl.semaphore_wait(barrier, 3)

    def span(c):
        if c == 0:
            return pl.ds(0, META + rows)
        return pl.ds(META + rows * c, rows)

    def ag_copy(src, k, c):
        return pltpu.make_async_remote_copy(
            src_ref=src.at[span(c)],
            dst_ref=ag.at[k, span(c)],
            send_sem=ag_ss.at[k],
            recv_sem=ag_rs.at[k, c],
            device_id={"ep": ahead},
            device_id_type=MESH,
        )

    for c in range(nch):
        ag_copy(own, 0, c).start()

    for copy in w_copies:
        copy.wait()

    @pl.when(tp == 0)
    def _():
        own_copy.wait()

    def x_copy(b):
        return pltpu.make_async_remote_copy(
            src_ref=x_own.at[b], dst_ref=x_sib.at[b], send_sem=x_ss.at[b],
            recv_sem=x_rs.at[b], device_id={"tp": sibling}, device_id_type=MESH,
        )

    def p_copy(b):
        return pltpu.make_async_remote_copy(
            src_ref=p_sib.at[b], dst_ref=p_rcv.at[b], send_sem=p_ss.at[b],
            recv_sem=p_rs.at[b], device_id={"tp": sibling}, device_id_type=MESH,
        )

    wide = BATCH * rows
    each = BATCH * cap

    def ag_step(b, j, c):
        k = b * BATCH + j
        if j < BATCH - 2:
            ag_copy(own, k, c).wait_recv()
            ag_copy(ag.at[k], k + 1, c).start()
        elif j == BATCH - 2:
            ag_copy(own, k, c).wait_recv()

            @pl.when(k <= reach - 2)
            def _():
                ag_copy(ag.at[k], k + 1, c).start()
        else:
            @pl.when(k <= reach - 1)
            def _():
                ag_copy(own, k, c).wait_recv()

            @pl.when(k <= reach - 2)
            def _():
                ag_copy(ag.at[k], k + 1, c).start()

    def routing(b):
        lane = lax.broadcasted_iota(jnp.int32, (META, wide), 1) // rows
        mm = ag[b * BATCH, 0:META, :].astype(F32)
        for j in range(1, BATCH):
            mm = jnp.where(lane == j, ag[b * BATCH + j, 0:META, :].astype(F32), mm)
        meta_s[...] = mm
        ids = [meta_s[k:k + 1, :] for k in range(4)]
        parts = [[meta_s[4 * (p + 1) + k:4 * (p + 1) + k + 1, :] for k in range(4)] for p in range(3)]
        row8 = lax.broadcasted_iota(jnp.int32, (8, wide), 0)
        members, gates = [], []
        for e in range(local):
            eid = (me * local + e).astype(F32)
            hits = [jnp.where(i == eid, 1.0, 0.0) for i in ids]
            members.append(sum(hits))
            gates.append([sum(h * g for h, g in zip(hits, part)) for part in parts])
        stacked = jnp.zeros((8, wide), F32)
        for e in range(local):
            stacked = jnp.where(row8 == e, members[e], stacked)
        rank_s[...] = dot(stacked.astype(BF16), upper[...])
        block = lax.broadcasted_iota(jnp.int32, (1, wide), 1) // rows
        row = lax.broadcasted_iota(jnp.int32, (each, wide), 0)
        for e in range(local):
            rank = rank_s[e:e + 1, :].astype(jnp.int32)
            key = jnp.where(members[e] > 0.5, block * cap + rank, -1)
            pick = jnp.where(row == key, 1.0, 0.0)
            sel[e * each:(e + 1) * each, :] = pick.astype(BF16)
            for p in range(3):
                at = (p * local + e) * each
                gsel[at:at + each, :] = (pick * gates[e][p]).astype(BF16)

    def select(b, c):
        block = jnp.concatenate(
            [ag[b * BATCH + j, META + rows * c:META + rows * (c + 1), :] for j in range(BATCH)], axis=0
        )
        x_own[b, :, c * CW:(c + 1) * CW] = dot(sel[...], block).astype(BF16)

    def expert_in(b, e):
        return jnp.concatenate(
            [x_own[b, e * each:(e + 1) * each, :], x_sib[b, e * each:(e + 1) * each, :]], axis=0
        )

    def gate_up(b, e):
        x = expert_in(b, e)
        gate = dot(x, wg[e])
        up = dot(x, wu[e])
        hid[e] = (gate / (1.0 + jnp.exp(-gate)) * up).astype(BF16)

    def down(b, e, part):
        cols = slice(part * width // 2, (part + 1) * width // 2)
        y = dot(hid[e], wd[e, :, cols]).astype(BF16)
        p_own[b, e * each:(e + 1) * each, cols] = y[:each]
        p_sib[b, e * each:(e + 1) * each, cols] = y[each:]

    def combine(b, c):
        cols = slice(c * CW, (c + 1) * CW)
        y = (p_own[b, :, cols].astype(F32) + p_rcv[b, :, cols].astype(F32)).astype(BF16)
        stacked = jnp.concatenate([y, y, y], axis=0)
        g = lax.dot_general(
            gsel[...], stacked, (((0,), (0,)), ((), ())), preferred_element_type=F32
        )
        for j in range(BATCH):
            contrib[b * BATCH + j, :, cols] = g[j * rows:(j + 1) * rows]

    def pieces(b):
        def start_x():
            for c in range(nch // 2, nch):
                select(b, c)
            x_copy(b).start()

        def first_half():
            for c in range(nch // 2):
                select(b, c)

        def wait_x():
            x_copy(b).wait_recv()
            gate_up(b, 0)

        def last_down():
            down(b, local - 1, 1)
            p_copy(b).start()

        def wait_p():
            p_copy(b).wait_recv()
            for c in range(nch // 2):
                combine(b, c)

        def rest():
            for c in range(nch // 2, nch):
                combine(b, c)

        return {
            0: functools.partial(routing, b),
            1: first_half,
            2: start_x,
            5: wait_x,
            6: functools.partial(down, b, 0, 0),
            7: functools.partial(down, b, 0, 1),
            8: functools.partial(gate_up, b, 1),
            9: functools.partial(down, b, 1, 0),
            10: last_down,
            14: wait_p,
            15: rest,
        }

    def window(b, _):
        work = pieces(b - 1)
        steps = [(j, c) for j in range(BATCH) for c in range(nch)]
        per = len(steps) // 16
        for i in range(16):
            @pl.when(b < batches)
            def _():
                for j, c in steps[i * per:(i + 1) * per]:
                    ag_step(b, j, c)

            if i in work:
                pl.when(b > 0)(work[i])
        return 0

    lax.fori_loop(0, batches + 1, window, 0)

    def rs_copy(src, d, c):
        return pltpu.make_async_remote_copy(
            src_ref=src.at[c],
            dst_ref=rs.at[d, c],
            send_sem=rs_ss.at[d],
            recv_sem=rs_rs.at[d, c],
            device_id={"ep": behind},
            device_id_type=MESH,
        )

    for c in range(nch):
        rs0[c] = contrib[reach - 1, :, c * CW:(c + 1) * CW].astype(BF16)
        rs_copy(rs0, reach - 1, c).start()

    def rs_step(i, _):
        d = reach - 1 - i

        @pl.when(d >= 1)
        def _():
            for c in range(nch):
                rs_copy(rs0, d, c).wait_recv()
                rs[d, c] = (
                    rs[d, c].astype(F32) + contrib[d - 1, :, c * CW:(c + 1) * CW]
                ).astype(BF16)
                rs_copy(rs.at[d], d - 1, c).start()
        return 0

    lax.fori_loop(0, slots - 1, rs_step, 0)

    share = (1 - tp).astype(F32)

    def f_copy(c):
        return pltpu.make_async_remote_copy(
            src_ref=rs.at[0, sibling * half_ch + c], dst_ref=fin.at[c], send_sem=f_ss.at[c],
            recv_sem=f_rs.at[c], device_id={"tp": sibling}, device_id_type=MESH,
        )

    for c in range(nch):
        rs_copy(rs0, 0, c).wait_recv()
    for c in range(half_ch):
        at = sibling * half_ch + c
        cols = pl.ds(pl.multiple_of(at * CW, CW), CW)
        rs[0, at] = (rs[0, at].astype(F32) + share * contrib[slots - 1, :, cols]).astype(BF16)
        f_copy(c).start()
    for c in range(half_ch):
        at = tp * half_ch + c
        cols = pl.ds(pl.multiple_of(at * CW, CW), CW)
        f_copy(c).wait_recv()
        out_ref[:, c * CW:(c + 1) * CW] = (
            rs[0, at].astype(F32) + share * contrib[slots - 1, :, cols] + fin[c].astype(F32)
        ).astype(BF16)

    def drain(k, _):
        @pl.when(k <= reach - 1)
        def _():
            pltpu.make_async_remote_copy(
                src_ref=ag.at[k], dst_ref=ag.at[k], send_sem=ag_ss.at[k], recv_sem=ag_rs.at[k, 0],
                device_id={"ep": ahead}, device_id_type=MESH,
            ).wait_send()
            pltpu.make_async_remote_copy(
                src_ref=rs.at[k], dst_ref=rs.at[k], send_sem=rs_ss.at[k], recv_sem=rs_rs.at[k, 0],
                device_id={"ep": behind}, device_id_type=MESH,
            ).wait_send()
        return 0

    lax.fori_loop(0, slots, drain, 0)
    for b in range(batches):
        x_copy(b).wait_send()
        p_copy(b).wait_send()
    for c in range(half_ch):
        f_copy(c).wait_send()


def on_device(tokens, norm_gain, groups, picks, gates, w_gate, w_up, w_down):
    rows, width = tokens.shape
    top = picks.shape[1]
    local, _, ffl = w_gate.shape
    n = lax.axis_size("ep")
    group_experts = n * local // GROUPS
    cap = rows * top // group_experts
    slots = n // 2
    batches = slots // BATCH
    nch = width // CW
    ids = (groups[:, None] * group_experts + picks).astype(F32)
    meta = jnp.concatenate([ids.T, gates.T, gates.T, gates.T], axis=0)
    meta = jnp.tile(meta, (1, BATCH))
    batch_rows = local * BATCH * cap
    vmem = pltpu.VMEM
    dma = pltpu.SemaphoreType.DMA
    return pl.pallas_call(
        functools.partial(kernel, n, rows, width, local, cap, ffl),
        out_shape=jax.ShapeDtypeStruct((rows, width // 2), BF16),
        in_specs=[pl.BlockSpec(memory_space=pltpu.VMEM)] * 3 + [pl.BlockSpec(memory_space=pl.ANY)] * 3,
        out_specs=pl.BlockSpec(memory_space=pltpu.VMEM),
        scratch_shapes=[
            vmem((META + rows * nch, CW), BF16),
            vmem((slots, META + rows * nch, CW), BF16),
            vmem((slots, nch, rows, CW), BF16),
            vmem((nch, rows, CW), BF16),
            vmem((slots, rows, width), F32),
            vmem(w_gate.shape, BF16),
            vmem(w_up.shape, BF16),
            vmem(w_down.shape, BF16),
            vmem((batches, batch_rows, width), BF16),
            vmem((batches, batch_rows, width), BF16),
            vmem((batches, batch_rows, width), BF16),
            vmem((batches, batch_rows, width), BF16),
            vmem((batches, batch_rows, width), BF16),
            vmem((nch // 2, rows, CW), BF16),
            vmem((batch_rows, BATCH * rows), BF16),
            vmem((3 * batch_rows, BATCH * rows), BF16),
            vmem((META, BATCH * rows), F32),
            vmem((8, BATCH * rows), F32),
            vmem((BATCH * rows, BATCH * rows), BF16),
            vmem((local, 2 * BATCH * cap, ffl), BF16),
            dma((slots,)), dma((slots, nch)), dma((slots,)), dma((slots, nch)),
            dma((batches,)), dma((batches,)), dma((batches,)), dma((batches,)),
            dma((nch // 2,)), dma((nch // 2,)), dma((3,)), dma,
        ],
        compiler_params=pltpu.CompilerParams(
            collective_id=0, has_side_effects=True, vmem_limit_bytes=60 * 2**20
        ),
    )(tokens, norm_gain.reshape(1, width), meta, w_gate, w_up, w_down)


def solution(mesh):
    in_specs = (
        P(("grp", "ep"), None),
        P(),
        P(("grp", "ep")),
        P(("grp", "ep"), None),
        P(("grp", "ep"), None),
        P("ep", None, "tp"),
        P("ep", None, "tp"),
        P("ep", "tp", None),
    )
    out_specs = P(("grp", "ep"), "tp")
    return jax.shard_map(
        on_device, mesh=mesh, in_specs=in_specs, out_specs=out_specs, check_vma=False
    )
```

```python
import functools

import jax
import jax.numpy as jnp
from jax import lax
from jax.experimental import pallas as pl
from jax.experimental.pallas import tpu as pltpu
from jax.sharding import PartitionSpec as P

GROUPS = 2
MESH = pl.DeviceIdType.MESH
F32 = jnp.float32
BF16 = jnp.bfloat16
CW = 256
META = 16
BATCH = 4

epsilon = 1e-06


def dot(a, b):
    return jnp.dot(a, b, preferred_element_type=F32)


def tdot(a, b):
    return lax.dot_general(a, b, (((0,), (0,)), ((), ())), preferred_element_type=F32)


def kernel(
    n, rows, width, local, cap, group_experts,
    tok_ref, gain_ref, grp_ref, pick_ref, gate_ref, wg_hbm, wu_hbm, wd_hbm, out_ref,
    own, ag, rs, rs0, contrib, wg, wu, wd, x_own, x_sib, p_own, p_sib, p_rcv, fin,
    sel, gsel, meta_s, rank_s, upper, hid, perm,
    ag_ss, ag_rs, rs_ss, rs_rs, x_ss, x_rs, p_ss, p_rs, f_ss, f_rs, w_sem, own_sem,
):
    slots = n // 2
    batches = slots // BATCH
    last = batches - 1
    nch = width // CW
    half_ch = nch // 2
    me = lax.axis_index("ep")
    tp = lax.axis_index("tp")
    right, left = lax.rem(me + 1, n), lax.rem(me + n - 1, n)
    ahead = jnp.where(tp == 1, right, left)
    behind = jnp.where(tp == 1, left, right)
    reach = slots - 1 + tp
    sibling = 1 - tp

    barrier = pltpu.get_barrier_semaphore()
    pl.semaphore_signal(barrier, inc=1, device_id={"ep": right}, device_id_type=MESH)
    pl.semaphore_signal(barrier, inc=1, device_id={"ep": left}, device_id_type=MESH)
    pl.semaphore_signal(barrier, inc=1, device_id={"tp": sibling}, device_id_type=MESH)

    w_copies = [
        pltpu.make_async_copy(src, dst, w_sem.at[i])
        for i, (src, dst) in enumerate(((wg_hbm, wg), (wu_hbm, wu), (wd_hbm, wd)))
    ]
    for copy in w_copies:
        copy.start()

    def need(k):
        return min(rows, local * cap * (slots - k))

    ri = lax.broadcasted_iota(jnp.int32, (rows, rows), 0)
    ci = lax.broadcasted_iota(jnp.int32, (rows, rows), 1)
    group = jnp.sum(jnp.where(ri == ci, grp_ref[...].astype(F32), 0.0), axis=1, keepdims=True)
    ids = group * group_experts + pick_ref[...].astype(F32)
    chip = lax.div(ids.astype(jnp.int32), jnp.full(ids.shape, local, jnp.int32))
    dist = (chip - me) * (2 * tp - 1) + n
    dist = jnp.where(dist >= n, dist - n, dist)
    dist = jnp.where(dist <= reach, dist, 0).astype(F32)
    far = jnp.max(dist, axis=1, keepdims=True)
    far_row = jnp.sum(jnp.where(ri == ci, far, 0.0), axis=0, keepdims=True)
    before = (far_row > far) | ((far_row == far) & (ci < ri))
    place = jnp.sum(jnp.where(before, 1.0, 0.0), axis=1, keepdims=True).astype(jnp.int32)
    lane = lax.rem(
        lax.broadcasted_iota(jnp.int32, (rows, BATCH * rows), 1),
        jnp.full((rows, BATCH * rows), rows, jnp.int32),
    )
    perm[...] = jnp.where(lane == place, 1.0, 0.0).astype(BF16)

    g = gate_ref[...]
    hi = g.astype(BF16).astype(F32)
    mid = (g - hi).astype(BF16).astype(F32)
    low = g - hi - mid
    for i, part in enumerate((ids, hi, mid, low)):
        meta_s[4 * i:4 * (i + 1), :] = tdot(part.astype(BF16), perm[...])
    own[0:META, :] = meta_s[...].astype(BF16)

    total = jnp.zeros((rows, 1), F32)
    for c in range(nch):
        v = tok_ref[:, c * CW:(c + 1) * CW].astype(F32)
        total = total + jnp.sum(v * v, axis=1, keepdims=True)
    scale = lax.rsqrt(total / width + epsilon)
    for c in range(nch):
        v = tok_ref[:, c * CW:(c + 1) * CW].astype(F32)
        normed = (v * scale * gain_ref[:, c * CW:(c + 1) * CW]).astype(BF16)
        own[META + rows * c:META + rows * (c + 1), :] = tdot(perm[:, 0:rows], normed).astype(BF16)

    for k in range(slots):
        if need(k) < rows:
            for c in range(nch):
                ag[k, META + rows * c + need(k):META + rows * (c + 1), :] = jnp.zeros(
                    (rows - need(k), CW), BF16
                )

    bi = lax.broadcasted_iota(jnp.int32, (BATCH * rows, BATCH * rows), 0)
    bj = lax.broadcasted_iota(jnp.int32, (BATCH * rows, BATCH * rows), 1)
    upper[...] = jnp.where((bi // rows == bj // rows) & (bi < bj), 1.0, 0.0).astype(BF16)

    own_copy = pltpu.make_async_copy(own, ag.at[0], own_sem)

    pl.semaphore_wait(barrier, 3)

    def span(c, count):
        if c == 0:
            return pl.ds(0, META + count)
        return pl.ds(META + rows * c, count)

    def ag_copy(src, k, c, count=rows):
        return pltpu.make_async_remote_copy(
            src_ref=src.at[span(c, count)],
            dst_ref=ag.at[k, span(c, count)],
            send_sem=ag_ss.at[k],
            recv_sem=ag_rs.at[k, c],
            device_id={"ep": ahead},
            device_id_type=MESH,
        )

    for c in range(nch):
        ag_copy(own, 1 - tp, c).start()

    @pl.when(tp == 0)
    def _():
        own_copy.start()
        own_copy.wait()

    half_cols = width // 2

    def x_copy(b, h):
        return pltpu.make_async_remote_copy(
            src_ref=x_own.at[b, h], dst_ref=x_sib.at[b, h], send_sem=x_ss.at[b, h],
            recv_sem=x_rs.at[b, h], device_id={"tp": sibling}, device_id_type=MESH,
        )

    def p_copy(b, h):
        return pltpu.make_async_remote_copy(
            src_ref=p_sib.at[b, h], dst_ref=p_rcv.at[b, h], send_sem=p_ss.at[b, h],
            recv_sem=p_rs.at[b, h], device_id={"tp": sibling}, device_id_type=MESH,
        )

    wide = BATCH * rows
    each = BATCH * cap

    def routing(b):
        lane = lax.broadcasted_iota(jnp.int32, (META, wide), 1) // rows
        mm = ag[b * BATCH, 0:META, :].astype(F32)
        for j in range(1, BATCH):
            mm = jnp.where(lane == j, ag[b * BATCH + j, 0:META, :].astype(F32), mm)
        meta_s[...] = mm
        ids = [meta_s[k:k + 1, :] for k in range(4)]
        parts = [[meta_s[4 * (p + 1) + k:4 * (p + 1) + k + 1, :] for k in range(4)] for p in range(3)]
        row8 = lax.broadcasted_iota(jnp.int32, (8, wide), 0)
        members, gates = [], []
        for e in range(local):
            eid = (me * local + e).astype(F32)
            hits = [jnp.where(i == eid, 1.0, 0.0) for i in ids]
            members.append(sum(hits))
            gates.append([sum(h * g for h, g in zip(hits, part)) for part in parts])
        stacked = jnp.zeros((8, wide), F32)
        for e in range(local):
            stacked = jnp.where(row8 == e, members[e], stacked)
        rank_s[...] = dot(stacked.astype(BF16), upper[...])
        block = lax.broadcasted_iota(jnp.int32, (1, wide), 1) // rows
        row = lax.broadcasted_iota(jnp.int32, (each, wide), 0)
        for e in range(local):
            rank = rank_s[e:e + 1, :].astype(jnp.int32)
            key = jnp.where(members[e] > 0.5, block * cap + rank, -1)
            pick = jnp.where(row == key, 1.0, 0.0)
            sel[e * each:(e + 1) * each, :] = pick.astype(BF16)
            for p in range(3):
                at = (p * local + e) * each
                gsel[at:at + each, :] = (pick * gates[e][p]).astype(BF16)

    def select(b, c):
        block = jnp.concatenate(
            [ag[b * BATCH + j, META + rows * c:META + rows * (c + 1), :] for j in range(BATCH)], axis=0
        )
        h, at = divmod(c, half_ch)
        x_own[b, h, :, at * CW:(at + 1) * CW] = dot(sel[...], block).astype(BF16)

    def expert_in(b, e, h):
        return jnp.concatenate(
            [x_own[b, h, e * each:(e + 1) * each, :], x_sib[b, h, e * each:(e + 1) * each, :]], axis=0
        )

    def gate_up(b, e):
        gate, up = 0.0, 0.0
        for h in range(2):
            x = expert_in(b, e, h)
            gate += dot(x, wg[e, h * half_cols:(h + 1) * half_cols, :])
            up += dot(x, wu[e, h * half_cols:(h + 1) * half_cols, :])
        hid[e] = (gate / (1.0 + jnp.exp(-gate)) * up).astype(BF16)

    def down(b, e, h):
        y = dot(hid[e], wd[e, :, h * half_cols:(h + 1) * half_cols]).astype(BF16)
        p_own[b, h, e * each:(e + 1) * each, :] = y[:each]
        p_sib[b, h, e * each:(e + 1) * each, :] = y[each:]

    def combine(b, c):
        h, at = divmod(c, half_ch)
        cols = slice(at * CW, (at + 1) * CW)
        y = (p_own[b, h, :, cols].astype(F32) + p_rcv[b, h, :, cols].astype(F32)).astype(BF16)
        g = tdot(gsel[...], jnp.concatenate([y, y, y], axis=0))
        for j in range(BATCH):
            contrib[b * BATCH + j, c] = g[j * rows:(j + 1) * rows]

    def run_all(*calls):
        def go():
            for call in calls:
                call()
        return go

    def pieces(b):
        call = functools.partial
        return {
            0: call(routing, b),
            1: run_all(*[call(select, b, c) for c in range(half_ch)], lambda: x_copy(b, 0).start()),
            2: run_all(*[call(select, b, c) for c in range(half_ch, nch)], lambda: x_copy(b, 1).start()),
            5: run_all(lambda: x_copy(b, 0).wait_recv(), lambda: x_copy(b, 1).wait_recv(), call(gate_up, b, 0)),
            6: call(down, b, 0, 0),
            7: call(down, b, 0, 1),
            8: call(gate_up, b, 1),
            9: run_all(call(down, b, 1, 0), lambda: p_copy(b, 0).start()),
            10: run_all(call(down, b, 1, 1), lambda: p_copy(b, 1).start()),
            14: run_all(lambda: p_copy(b, 0).wait_recv(), *[call(combine, b, c) for c in range(half_ch)]),
            15: run_all(lambda: p_copy(b, 1).wait_recv(), *[call(combine, b, c) for c in range(half_ch, nch)]),
        }

    def ag_step(b, j, c, final):
        k = b * BATCH + j
        if final:
            k = last * BATCH + j
            ag_copy(own, k, c, need(k)).wait_recv()
            if k < slots - 1:
                ag_copy(ag.at[k], k + 1, c, need(k + 1)).start()
        elif j == 0:
            @pl.when(k + tp >= 1)
            def _():
                ag_copy(own, k, c).wait_recv()
                ag_copy(ag.at[k], k + 1, c).start()
        else:
            ag_copy(own, k, c).wait_recv()
            ag_copy(ag.at[k], k + 1, c).start()

    order = [(j, c) for j in range(BATCH) for c in range(nch)]
    per = len(order) // 16

    def window(b, _):
        work = pieces(b - 1)
        for i in range(16):
            for j, c in order[i * per:(i + 1) * per]:
                ag_step(b, j, c, False)
            if i in work:
                pl.when(b > 0)(work[i])
            if i == 4:
                @pl.when(b == 1)
                def _():
                    for copy in w_copies:
                        copy.wait()
        return 0

    lax.fori_loop(0, last, window, 0)

    work = pieces(last - 1)
    for i in range(16):
        for j, c in order[i * per:(i + 1) * per]:
            if j == BATCH - 1:
                continue
            ag_step(last, j, c, True)
        if i in work and i < 14:
            work[i]()
    work[14]()
    work[15]()

    for c in range(nch):
        ag_step(last, BATCH - 1, c, True)
        if c == 0:
            routing(last)
        select(last, c)
        if c in (half_ch - 1, nch - 1):
            x_copy(last, c // half_ch).start()
    partial = {}
    for h in range(2):
        x_copy(last, h).wait_recv()
        for e in range(local):
            x = expert_in(last, e, h)
            for i, w in enumerate((wg, wu)):
                y = dot(x, w[e, h * half_cols:(h + 1) * half_cols, :])
                partial[e, i] = y if h == 0 else partial[e, i] + y
    for e in range(local):
        gate, up = partial[e, 0], partial[e, 1]
        hid[e] = (gate / (1.0 + jnp.exp(-gate)) * up).astype(BF16)
    for h in range(2):
        for e in range(local):
            down(last, e, h)
        p_copy(last, h).start()

    def rs_copy(src, k, at, count=rows):
        return pltpu.make_async_remote_copy(
            src_ref=src.at[at, pl.ds(0, count)],
            dst_ref=rs.at[k, at, pl.ds(0, count)],
            send_sem=rs_ss.at[k],
            recv_sem=rs_rs.at[k, at],
            device_id={"ep": behind},
            device_id_type=MESH,
        )

    def turn(c):
        at = c + sibling * half_ch
        return jnp.where(at >= nch, at - nch, at)

    for h in range(2):
        p_copy(last, h).wait_recv()
        for c in range(h * half_ch, (h + 1) * half_ch):
            combine(last, c)
            count = need(slots - 1)
            rs0[c] = contrib[slots - 1, c].astype(BF16)
            rs_copy(rs0, slots - 2, c, count).start()

    def rs_step(k, got, count):
        for c in range(nch):
            at = turn(c)
            rs_copy(rs0, k, at, got).wait_recv()
            rs[k, at, 0:got, :] = (
                rs[k, at, 0:got, :].astype(F32) + contrib[k, at, 0:got, :]
            ).astype(BF16)
            if got < count:
                rs[k, at, got:count, :] = contrib[k, at, got:count, :].astype(BF16)
            rs_copy(rs.at[k], k - 1, at, count).start()

    k = slots - 2
    while need(k + 1) < rows:
        rs_step(k, need(k + 1), need(k))
        k -= 1
    top_k = k

    def rs_loop(i, _):
        rs_step(top_k - i, rows, rows)
        return 0

    lax.fori_loop(0, top_k, rs_loop, 0)

    @pl.when(tp == 1)
    def _():
        for c in range(nch):
            at = turn(c)
            rs_copy(rs0, 0, at).wait_recv()
            rs[0, at] = (rs[0, at].astype(F32) + contrib[0, at]).astype(BF16)
            rs_copy(rs.at[0], slots, at).start()
    end = jnp.where(tp == 1, slots, 0)
    share = (1 - tp).astype(F32)

    def f_copy(c):
        return pltpu.make_async_remote_copy(
            src_ref=rs0.at[c], dst_ref=fin.at[c], send_sem=f_ss.at[c],
            recv_sem=f_rs.at[c], device_id={"tp": sibling}, device_id_type=MESH,
        )

    rs0_sent = pltpu.make_async_remote_copy(
        src_ref=rs0.at[:, pl.ds(0, need(slots - 1))], dst_ref=rs0.at[:, pl.ds(0, need(slots - 1))],
        send_sem=rs_ss.at[slots - 2], recv_sem=rs_rs.at[slots - 2, 0],
        device_id={"ep": behind}, device_id_type=MESH,
    )
    rs0_sent.wait_send()
    for c in range(nch):
        at = turn(c)
        rs_copy(rs0, end, at).wait_recv()
        v = (rs[end, at].astype(F32) + share * contrib[0, at]).astype(BF16)
        y = dot(perm[:, 0:rows], v)
        if c < half_ch:
            rs0[c] = y.astype(BF16)
            f_copy(c).start()
        else:
            i = c - half_ch
            f_copy(i).wait_recv()
            out_ref[:, i * CW:(i + 1) * CW] = (y + fin[i].astype(F32)).astype(BF16)

    def ag_sent(k, count):
        size = pl.ds(0, META + nch * count)
        pltpu.make_async_remote_copy(
            src_ref=ag.at[k, size], dst_ref=ag.at[k, size], send_sem=ag_ss.at[k],
            recv_sem=ag_rs.at[k, 0], device_id={"ep": ahead}, device_id_type=MESH,
        ).wait_send()

    def rs_sent(k, count):
        size = pl.ds(0, count)
        pltpu.make_async_remote_copy(
            src_ref=rs.at[k, :, size], dst_ref=rs.at[k, :, size], send_sem=rs_ss.at[k],
            recv_sem=rs_rs.at[k, 0], device_id={"ep": behind}, device_id_type=MESH,
        ).wait_send()

    @pl.when(tp == 1)
    def _():
        ag_sent(0, rows)
        rs_sent(slots, rows)

    for k in range(1, slots):
        ag_sent(k, need(k))
    for k in range(slots - 2):
        rs_sent(k, need(k + 1))
    for b in range(batches):
        for h in range(2):
            x_copy(b, h).wait_send()
            p_copy(b, h).wait_send()
    for c in range(half_ch):
        f_copy(c).wait_send()


def on_device(tokens, norm_gain, groups, picks, gates, w_gate, w_up, w_down):
    rows, width = tokens.shape
    top = picks.shape[1]
    local, _, ffl = w_gate.shape
    n = lax.axis_size("ep")
    group_experts = n * local // GROUPS
    cap = rows * top // group_experts
    slots = n // 2
    batches = slots // BATCH
    nch = width // CW
    batch_rows = local * BATCH * cap
    vmem = pltpu.VMEM
    dma = pltpu.SemaphoreType.DMA
    return pl.pallas_call(
        functools.partial(kernel, n, rows, width, local, cap, group_experts),
        out_shape=jax.ShapeDtypeStruct((rows, width // 2), BF16),
        in_specs=[pl.BlockSpec(memory_space=pltpu.VMEM)] * 5 + [pl.BlockSpec(memory_space=pl.ANY)] * 3,
        out_specs=pl.BlockSpec(memory_space=pltpu.VMEM),
        scratch_shapes=[
            vmem((META + rows * nch, CW), BF16),
            vmem((slots, META + rows * nch, CW), BF16),
            vmem((slots + 1, nch, rows, CW), BF16),
            vmem((nch, rows, CW), BF16),
            vmem((slots, nch, rows, CW), F32),
            vmem(w_gate.shape, BF16),
            vmem(w_up.shape, BF16),
            vmem(w_down.shape, BF16),
            vmem((batches, 2, batch_rows, width // 2), BF16),
            vmem((batches, 2, batch_rows, width // 2), BF16),
            vmem((batches, 2, batch_rows, width // 2), BF16),
            vmem((batches, 2, batch_rows, width // 2), BF16),
            vmem((batches, 2, batch_rows, width // 2), BF16),
            vmem((nch // 2, rows, CW), BF16),
            vmem((batch_rows, BATCH * rows), BF16),
            vmem((3 * batch_rows, BATCH * rows), BF16),
            vmem((META, BATCH * rows), F32),
            vmem((8, BATCH * rows), F32),
            vmem((BATCH * rows, BATCH * rows), BF16),
            vmem((local, 2 * BATCH * cap, ffl), BF16),
            vmem((rows, BATCH * rows), BF16),
            dma((slots,)), dma((slots, nch)), dma((slots + 1,)), dma((slots + 1, nch)),
            dma((batches, 2)), dma((batches, 2)), dma((batches, 2)), dma((batches, 2)),
            dma((nch // 2,)), dma((nch // 2,)), dma((3,)), dma,
        ],
        compiler_params=pltpu.CompilerParams(
            collective_id=0, has_side_effects=True, vmem_limit_bytes=60 * 2**20
        ),
    )(
        tokens, norm_gain.reshape(1, width), groups.reshape(1, rows), picks, gates,
        w_gate, w_up, w_down,
    )


def solution(mesh):
    in_specs = (
        P(("grp", "ep"), None),
        P(),
        P(("grp", "ep")),
        P(("grp", "ep"), None),
        P(("grp", "ep"), None),
        P("ep", None, "tp"),
        P("ep", None, "tp"),
        P("ep", "tp", None),
    )
    out_specs = P(("grp", "ep"), "tp")
    return jax.shard_map(
        on_device, mesh=mesh, in_specs=in_specs, out_specs=out_specs, check_vma=False
    )
```

```python
import functools

import jax
import jax.numpy as jnp
from jax import lax
from jax.experimental import pallas as pl
from jax.experimental.pallas import tpu as pltpu
from jax.sharding import PartitionSpec as P

GROUPS = 2
MESH = pl.DeviceIdType.MESH
F32 = jnp.float32
BF16 = jnp.bfloat16
CW = 256
META = 16
BATCH = 4

epsilon = 1e-06


def dot(a, b):
    return jnp.dot(a, b, preferred_element_type=F32)


def tdot(a, b):
    return lax.dot_general(a, b, (((0,), (0,)), ((), ())), preferred_element_type=F32)


def kernel(
    n, rows, width, local, cap, group_experts,
    tok_ref, gain_ref, grp_ref, pick_ref, gate_ref, wg_hbm, wu_hbm, wd_hbm, out_ref,
    own, ag, rs, rs0, contrib, wg, wu, wd, x_own, x_sib, p_own, p_sib, p_rcv, fin,
    sel, gsel, meta_s, rank_s, upper, hid, perm,
    ag_ss, got, rs_ss, x_ss, x_rs, p_ss, p_rs, f_ss, f_rs, w_sem, own_sem,
):
    slots = n // 2
    batches = slots // BATCH
    last = batches - 1
    nch = width // CW
    half_ch = nch // 2
    me = lax.axis_index("ep")
    tp = lax.axis_index("tp")
    right, left = lax.rem(me + 1, n), lax.rem(me + n - 1, n)
    ahead = jnp.where(tp == 1, right, left)
    behind = jnp.where(tp == 1, left, right)
    reach = slots - 1 + tp
    sibling = 1 - tp

    barrier = pltpu.get_barrier_semaphore()
    pl.semaphore_signal(barrier, inc=1, device_id={"ep": right}, device_id_type=MESH)
    pl.semaphore_signal(barrier, inc=1, device_id={"ep": left}, device_id_type=MESH)
    pl.semaphore_signal(barrier, inc=1, device_id={"tp": sibling}, device_id_type=MESH)

    w_copies = [
        pltpu.make_async_copy(src, dst, w_sem.at[i])
        for i, (src, dst) in enumerate(((wg_hbm, wg), (wu_hbm, wu), (wd_hbm, wd)))
    ]
    for copy in w_copies:
        copy.start()

    split = rows // 2

    def parts(count):
        return [(lo, min(count, lo + split)) for lo in range(0, count, split)]

    def need(k):
        return min(rows, local * cap * (slots - k))

    ri = lax.broadcasted_iota(jnp.int32, (rows, rows), 0)
    ci = lax.broadcasted_iota(jnp.int32, (rows, rows), 1)
    ids = grp_ref[...] * group_experts + pick_ref[...]
    chip = lax.div(ids, jnp.full(ids.shape, local, jnp.int32))
    dist = (chip - me) * (2 * tp - 1) + n
    dist = jnp.where(dist >= n, dist - n, dist)
    dist = jnp.where(dist <= reach, dist, 0).astype(F32)
    far_row = jnp.max(dist, axis=0, keepdims=True)
    far = jnp.sum(jnp.where(ri == ci, far_row, 0.0), axis=1, keepdims=True)
    before = (far_row > far) | ((far_row == far) & (ci < ri))
    place = jnp.sum(jnp.where(before, 1.0, 0.0), axis=1, keepdims=True).astype(jnp.int32)
    lane = lax.rem(
        lax.broadcasted_iota(jnp.int32, (rows, BATCH * rows), 1),
        jnp.full((rows, BATCH * rows), rows, jnp.int32),
    )
    perm[...] = jnp.where(lane == place, 1.0, 0.0).astype(BF16)

    g = gate_ref[...]
    hi = g.astype(BF16).astype(F32)
    mid = (g - hi).astype(BF16).astype(F32)
    low = g - hi - mid
    for i, part in enumerate((ids.astype(F32), hi, mid, low)):
        meta_s[4 * i:4 * (i + 1), :] = dot(part.astype(BF16), perm[...])
    own[0:META, :] = meta_s[...].astype(BF16)

    total = jnp.zeros((rows, CW), F32)
    for c in range(nch):
        v = tok_ref[:, c * CW:(c + 1) * CW].astype(F32)
        total = total + v * v
    scale = lax.rsqrt(jnp.sum(total, axis=1, keepdims=True) / width + epsilon)

    def ag_copy(src, k, c, part):
        lo, hi = part
        first = 0 if c == 0 and lo == 0 else META + rows * c + lo
        span = pl.ds(first, META + rows * c + hi - first)
        return pltpu.make_async_remote_copy(
            src_ref=src.at[span],
            dst_ref=ag.at[k, span],
            send_sem=ag_ss.at[k],
            recv_sem=got.at[k, c, lo // split],
            device_id={"ep": ahead},
            device_id_type=MESH,
        )

    pl.semaphore_wait(barrier, 3)
    for c in range(nch):
        v = tok_ref[:, c * CW:(c + 1) * CW].astype(F32)
        normed = (v * scale * gain_ref[:, c * CW:(c + 1) * CW]).astype(BF16)
        own[META + rows * c:META + rows * (c + 1), :] = tdot(perm[:, 0:rows], normed).astype(BF16)
        for part in parts(rows):
            ag_copy(own, 1 - tp, c, part).start()

    own_copy = pltpu.make_async_copy(own, ag.at[0], own_sem)

    @pl.when(tp == 0)
    def _():
        own_copy.start()

    for k in range(slots):
        if need(k) < rows:
            for c in range(nch):
                ag[k, META + rows * c + need(k):META + rows * (c + 1), :] = jnp.zeros(
                    (rows - need(k), CW), BF16
                )

    bi = lax.broadcasted_iota(jnp.int32, (BATCH * rows, BATCH * rows), 0)
    bj = lax.broadcasted_iota(jnp.int32, (BATCH * rows, BATCH * rows), 1)
    upper[...] = jnp.where((bi // rows == bj // rows) & (bi < bj), 1.0, 0.0).astype(BF16)

    @pl.when(tp == 0)
    def _():
        own_copy.wait()

    half_cols = width // 2

    def x_copy(b, h):
        return pltpu.make_async_remote_copy(
            src_ref=x_own.at[b, h], dst_ref=x_sib.at[b, h], send_sem=x_ss.at[b, h],
            recv_sem=x_rs.at[b, h], device_id={"tp": sibling}, device_id_type=MESH,
        )

    def p_copy(b, h):
        return pltpu.make_async_remote_copy(
            src_ref=p_sib.at[b, h], dst_ref=p_rcv.at[b, h], send_sem=p_ss.at[b, h],
            recv_sem=p_rs.at[b, h], device_id={"tp": sibling}, device_id_type=MESH,
        )

    wide = BATCH * rows
    each = BATCH * cap

    def routing(b):
        lane = lax.broadcasted_iota(jnp.int32, (META, wide), 1) // rows
        mm = ag[b * BATCH, 0:META, :].astype(F32)
        for j in range(1, BATCH):
            mm = jnp.where(lane == j, ag[b * BATCH + j, 0:META, :].astype(F32), mm)
        meta_s[...] = mm
        ids = [meta_s[k:k + 1, :] for k in range(4)]
        parts = [[meta_s[4 * (p + 1) + k:4 * (p + 1) + k + 1, :] for k in range(4)] for p in range(3)]
        row8 = lax.broadcasted_iota(jnp.int32, (8, wide), 0)
        members, gates = [], []
        for e in range(local):
            eid = (me * local + e).astype(F32)
            hits = [jnp.where(i == eid, 1.0, 0.0) for i in ids]
            members.append(sum(hits))
            gates.append([sum(h * g for h, g in zip(hits, part)) for part in parts])
        stacked = jnp.zeros((8, wide), F32)
        for e in range(local):
            stacked = jnp.where(row8 == e, members[e], stacked)
        rank_s[...] = dot(stacked.astype(BF16), upper[...])
        block = lax.broadcasted_iota(jnp.int32, (1, wide), 1) // rows
        row = lax.broadcasted_iota(jnp.int32, (each, wide), 0)
        for e in range(local):
            rank = rank_s[e:e + 1, :].astype(jnp.int32)
            key = jnp.where(members[e] > 0.5, block * cap + rank, -1)
            pick = jnp.where(row == key, 1.0, 0.0)
            sel[e * each:(e + 1) * each, :] = pick.astype(BF16)
            for p in range(3):
                at = (p * local + e) * each
                gsel[at:at + each, :] = (pick * gates[e][p]).astype(BF16)

    def select(b, c):
        block = jnp.concatenate(
            [ag[b * BATCH + j, META + rows * c:META + rows * (c + 1), :] for j in range(BATCH)], axis=0
        )
        h, at = divmod(c, half_ch)
        x_own[b, h, :, at * CW:(at + 1) * CW] = dot(sel[...], block).astype(BF16)

    def expert_in(b, e, h):
        return jnp.concatenate(
            [x_own[b, h, e * each:(e + 1) * each, :], x_sib[b, h, e * each:(e + 1) * each, :]], axis=0
        )

    def gate_up(b, e):
        gate, up = 0.0, 0.0
        for h in range(2):
            x = expert_in(b, e, h)
            gate += dot(x, wg[e, h * half_cols:(h + 1) * half_cols, :])
            up += dot(x, wu[e, h * half_cols:(h + 1) * half_cols, :])
        hid[e] = (gate / (1.0 + jnp.exp(-gate)) * up).astype(BF16)

    def down(b, e, h):
        y = dot(hid[e], wd[e, :, h * half_cols:(h + 1) * half_cols]).astype(BF16)
        p_own[b, h, e * each:(e + 1) * each, :] = y[:each]
        p_sib[b, h, e * each:(e + 1) * each, :] = y[each:]

    def combine(b, c):
        h, at = divmod(c, half_ch)
        cols = slice(at * CW, (at + 1) * CW)
        y = (p_own[b, h, :, cols].astype(F32) + p_rcv[b, h, :, cols].astype(F32)).astype(BF16)
        g = tdot(gsel[...], jnp.concatenate([y, y, y], axis=0))
        for j in range(BATCH):
            contrib[b * BATCH + j, c] = g[j * rows:(j + 1) * rows]

    def run_all(*calls):
        def go():
            for call in calls:
                call()
        return go

    def pieces(b):
        call = functools.partial
        return {
            0: call(routing, b),
            1: run_all(*[call(select, b, c) for c in range(half_ch)], lambda: x_copy(b, 0).start()),
            2: run_all(*[call(select, b, c) for c in range(half_ch, nch)], lambda: x_copy(b, 1).start()),
            5: run_all(lambda: x_copy(b, 0).wait_recv(), lambda: x_copy(b, 1).wait_recv(), call(gate_up, b, 0)),
            6: call(down, b, 0, 0),
            7: call(down, b, 0, 1),
            8: call(gate_up, b, 1),
            9: run_all(call(down, b, 1, 0), lambda: p_copy(b, 0).start()),
            10: run_all(call(down, b, 1, 1), lambda: p_copy(b, 1).start()),
            14: run_all(lambda: p_copy(b, 0).wait_recv(), *[call(combine, b, c) for c in range(half_ch)]),
            15: run_all(lambda: p_copy(b, 1).wait_recv(), *[call(combine, b, c) for c in range(half_ch, nch)]),
        }

    def ag_step(b, j, c, final):
        k = b * BATCH + j

        def both(k, count, ahead_count):
            for part in parts(count):
                ag_copy(own, k, c, part).wait_recv()
                if part[0] < ahead_count:
                    part = (part[0], min(part[1], ahead_count))
                    ag_copy(ag.at[k], k + 1, c, part).start()

        if final:
            k = last * BATCH + j
            both(k, need(k), need(k + 1) if k < slots - 1 else 0)
        elif j == 0:
            pl.when(k + tp >= 1)(lambda: both(k, rows, rows))
        else:
            both(k, rows, rows)

    order = [(j, c) for j in range(BATCH) for c in range(nch)]
    per = len(order) // 16

    def window(b, _):
        work = pieces(b - 1)
        for i in range(16):
            for j, c in order[i * per:(i + 1) * per]:
                ag_step(b, j, c, False)
            if i in work:
                pl.when(b > 0)(work[i])
            if i == 4:
                @pl.when(b == 1)
                def _():
                    for copy in w_copies:
                        copy.wait()
        return 0

    lax.fori_loop(0, last, window, 0)

    work = pieces(last - 1)
    for i in range(16):
        for j, c in order[i * per:(i + 1) * per]:
            if j == BATCH - 1:
                continue
            ag_step(last, j, c, True)
        if i in work and i < 14:
            work[i]()
    work[14]()
    work[15]()

    for c in range(nch):
        ag_step(last, BATCH - 1, c, True)
        if c == 0:
            routing(last)
        select(last, c)
        if c in (half_ch - 1, nch - 1):
            x_copy(last, c // half_ch).start()
    partial = {}
    for h in range(2):
        x_copy(last, h).wait_recv()
        for e in range(local):
            x = expert_in(last, e, h)
            for i, w in enumerate((wg, wu)):
                y = dot(x, w[e, h * half_cols:(h + 1) * half_cols, :])
                partial[e, i] = y if h == 0 else partial[e, i] + y
    for e in range(local):
        gate, up = partial[e, 0], partial[e, 1]
        hid[e] = (gate / (1.0 + jnp.exp(-gate)) * up).astype(BF16)
    for h in range(2):
        for e in range(local):
            down(last, e, h)
        p_copy(last, h).start()

    def rs_copy(src, k, at, part):
        span = pl.ds(part[0], part[1] - part[0])
        return pltpu.make_async_remote_copy(
            src_ref=src.at[at, span],
            dst_ref=rs.at[k, at, span],
            send_sem=rs_ss.at[k],
            recv_sem=got.at[k, at, part[0] // split],
            device_id={"ep": behind},
            device_id_type=MESH,
        )

    def turn(c):
        at = c + sibling * half_ch
        return jnp.where(at >= nch, at - nch, at)

    for h in range(2):
        p_copy(last, h).wait_recv()
        for c in range(h * half_ch, (h + 1) * half_ch):
            combine(last, c)
            count = need(slots - 1)
            rs0[c] = contrib[slots - 1, c].astype(BF16)
            for part in parts(count):
                rs_copy(rs0, slots - 2, c, part).start()

    def rs_add(k, to, at, there, count):
        for lo, hi in parts(count):
            mid = max(lo, min(hi, there))
            if lo < mid:
                rs_copy(rs0, k, at, (lo, mid)).wait_recv()
                rs[k, at, lo:mid, :] = (
                    rs[k, at, lo:mid, :].astype(F32) + contrib[k, at, lo:mid, :]
                ).astype(BF16)
            if mid < hi:
                rs[k, at, mid:hi, :] = contrib[k, at, mid:hi, :].astype(BF16)
            rs_copy(rs.at[k], to, at, (lo, hi)).start()

    def rs_step(k, there, count):
        for c in range(nch):
            rs_add(k, k - 1, turn(c), there, count)

    k = slots - 2
    while need(k + 1) < rows:
        rs_step(k, need(k + 1), need(k))
        k -= 1
    top_k = k

    def rs_loop(i, _):
        rs_step(top_k - i, rows, rows)
        return 0

    lax.fori_loop(0, top_k, rs_loop, 0)

    @pl.when(tp == 1)
    def _():
        for c in range(nch):
            rs_add(0, slots, turn(c), rows, rows)
    def ag_sent(k, count):
        size = pl.ds(0, META + nch * count)
        pltpu.make_async_remote_copy(
            src_ref=ag.at[k, size], dst_ref=ag.at[k, size], send_sem=ag_ss.at[k],
            recv_sem=got.at[k, 0, 0], device_id={"ep": ahead}, device_id_type=MESH,
        ).wait_send()

    def rs_sent(k, count):
        size = pl.ds(0, count)
        pltpu.make_async_remote_copy(
            src_ref=rs.at[k, :, size], dst_ref=rs.at[k, :, size], send_sem=rs_ss.at[k],
            recv_sem=got.at[k, 0, 0], device_id={"ep": behind}, device_id_type=MESH,
        ).wait_send()

    pl.when(tp == 1)(functools.partial(ag_sent, 0, rows))
    for k in range(1, slots):
        ag_sent(k, need(k))
    for b in range(batches):
        for h in range(2):
            x_copy(b, h).wait_send()
            p_copy(b, h).wait_send()
    for k in range(3, slots - 2):
        rs_sent(k, need(k + 1))

    end = jnp.where(tp == 1, slots, 0)
    share = (1 - tp).astype(F32)

    def f_copy(c):
        return pltpu.make_async_remote_copy(
            src_ref=rs0.at[c], dst_ref=fin.at[c], send_sem=f_ss.at[c],
            recv_sem=f_rs.at[c], device_id={"tp": sibling}, device_id_type=MESH,
        )

    rs0_sent = pltpu.make_async_remote_copy(
        src_ref=rs0.at[:, pl.ds(0, need(slots - 1))], dst_ref=rs0.at[:, pl.ds(0, need(slots - 1))],
        send_sem=rs_ss.at[slots - 2], recv_sem=got.at[slots - 2, 0, 0],
        device_id={"ep": behind}, device_id_type=MESH,
    )
    rs0_sent.wait_send()
    for c in range(nch):
        at = turn(c)
        for part in parts(rows):
            rs_copy(rs0, end, at, part).wait_recv()
        v = (rs[end, at].astype(F32) + share * contrib[0, at]).astype(BF16)
        y = dot(perm[:, 0:rows], v)
        if c < half_ch:
            rs0[c] = y.astype(BF16)
            f_copy(c).start()
        else:
            i = c - half_ch
            f_copy(i).wait_recv()
            out_ref[:, i * CW:(i + 1) * CW] = (y + fin[i].astype(F32)).astype(BF16)

    for k in range(3):
        rs_sent(k, need(k + 1))

    @pl.when(tp == 1)
    def _():
        rs_sent(slots, rows)

    for c in range(half_ch):
        f_copy(c).wait_send()


def on_device(tokens, norm_gain, groups, picks, gates, w_gate, w_up, w_down):
    rows, width = tokens.shape
    top = picks.shape[1]
    local, _, ffl = w_gate.shape
    n = lax.axis_size("ep")
    group_experts = n * local // GROUPS
    cap = rows * top // group_experts
    slots = n // 2
    batches = slots // BATCH
    nch = width // CW
    batch_rows = local * BATCH * cap
    vmem = pltpu.VMEM
    dma = pltpu.SemaphoreType.DMA
    return pl.pallas_call(
        functools.partial(kernel, n, rows, width, local, cap, group_experts),
        out_shape=pltpu.VMEM((rows, width // 2), BF16),
        in_specs=[pl.BlockSpec(memory_space=pltpu.VMEM)] * 5 + [pl.BlockSpec(memory_space=pl.ANY)] * 3,
        out_specs=pl.BlockSpec(memory_space=pltpu.VMEM),
        scratch_shapes=[
            vmem((META + rows * nch, CW), BF16),
            vmem((slots, META + rows * nch, CW), BF16),
            vmem((slots + 1, nch, rows, CW), BF16),
            vmem((nch, rows, CW), BF16),
            vmem((slots, nch, rows, CW), F32),
            vmem(w_gate.shape, BF16),
            vmem(w_up.shape, BF16),
            vmem(w_down.shape, BF16),
            vmem((batches, 2, batch_rows, width // 2), BF16),
            vmem((batches, 2, batch_rows, width // 2), BF16),
            vmem((batches, 2, batch_rows, width // 2), BF16),
            vmem((batches, 2, batch_rows, width // 2), BF16),
            vmem((batches, 2, batch_rows, width // 2), BF16),
            vmem((nch // 2, rows, CW), BF16),
            vmem((batch_rows, BATCH * rows), BF16),
            vmem((3 * batch_rows, BATCH * rows), BF16),
            vmem((META, BATCH * rows), F32),
            vmem((8, BATCH * rows), F32),
            vmem((BATCH * rows, BATCH * rows), BF16),
            vmem((local, 2 * BATCH * cap, ffl), BF16),
            vmem((rows, BATCH * rows), BF16),
            dma((slots,)), dma((slots + 1, nch, 2)), dma((slots + 1,)),
            dma((batches, 2)), dma((batches, 2)), dma((batches, 2)), dma((batches, 2)),
            dma((nch // 2,)), dma((nch // 2,)), dma((3,)), dma,
        ],
        compiler_params=pltpu.CompilerParams(
            collective_id=0, has_side_effects=True, vmem_limit_bytes=60 * 2**20
        ),
    )(
        tokens, norm_gain.reshape(1, width), groups.reshape(1, rows), picks.T, gates.T,
        w_gate, w_up, w_down,
    )


def solution(mesh):
    in_specs = (
        P(("grp", "ep"), None),
        P(),
        P(("grp", "ep")),
        P(("grp", "ep"), None),
        P(("grp", "ep"), None),
        P("ep", None, "tp"),
        P("ep", None, "tp"),
        P("ep", "tp", None),
    )
    out_specs = P(("grp", "ep"), "tp")
    return jax.shard_map(
        on_device, mesh=mesh, in_specs=in_specs, out_specs=out_specs, check_vma=False
    )
```

```python
import functools

import jax
import jax.numpy as jnp
from jax import lax
from jax.experimental import pallas as pl
from jax.experimental.pallas import tpu as pltpu
from jax.sharding import PartitionSpec as P

GROUPS = 2
MESH = pl.DeviceIdType.MESH
F32 = jnp.float32
BF16 = jnp.bfloat16
CW = 256
LANES = 128
META = 16
BATCH = 4

epsilon = 1e-06


def dot(a, b):
    return jnp.dot(a, b, preferred_element_type=F32)


def tdot(a, b):
    return lax.dot_general(a, b, (((0,), (0,)), ((), ())), preferred_element_type=F32)


def kernel(
    n, rows, width, local, cap, group_experts,
    tok_ref, gain_ref, grp_ref, pick_ref, gate_ref, wg_hbm, wu_hbm, wd_hbm, out_ref,
    own, ag, rs, rs0, contrib, wg, wu, wd, x_own, x_sib, p_own, p_sib, p_rcv, fin,
    sel, gsel, meta_s, rank_s, upper, hid, perm, skip,
    ag_ss, got, rs_ss, x_ss, x_rs, p_ss, p_rs, f_ss, f_rs, w_sem, own_sem,
):
    slots = n // 2
    batches = slots // BATCH
    last = batches - 1
    nch = width // CW
    half_ch = nch // 2
    fine = width // LANES
    me = lax.axis_index("ep")
    tp = lax.axis_index("tp")
    right, left = lax.rem(me + 1, n), lax.rem(me + n - 1, n)
    ahead = jnp.where(tp == 1, right, left)
    behind = jnp.where(tp == 1, left, right)
    ahead2 = lax.rem(ahead + ahead - me + n, n)
    behind2 = lax.rem(behind + behind - me + n, n)
    reach = slots - 1 + tp
    sibling = 1 - tp

    barrier = pltpu.get_barrier_semaphore()
    for peer in (ahead2, behind2, ahead, behind):
        pl.semaphore_signal(barrier, inc=1, device_id={"ep": peer}, device_id_type=MESH)
    pl.semaphore_signal(barrier, inc=1, device_id={"tp": sibling}, device_id_type=MESH)

    w_copies = [
        pltpu.make_async_copy(src, dst, w_sem.at[i])
        for i, (src, dst) in enumerate(((wg_hbm, wg), (wu_hbm, wu), (wd_hbm, wd)))
    ]
    for copy in w_copies:
        copy.start()

    split = rows // 2

    def parts(count):
        return [(lo, min(count, lo + split)) for lo in range(0, count, split)]

    def need(k):
        return min(rows, local * cap * (slots - k))

    ri = lax.broadcasted_iota(jnp.int32, (rows, rows), 0)
    ci = lax.broadcasted_iota(jnp.int32, (rows, rows), 1)
    ids = grp_ref[...] * group_experts + pick_ref[...]
    chip = lax.div(ids, jnp.full(ids.shape, local, jnp.int32))
    dist = (chip - me) * (2 * tp - 1) + n
    dist = jnp.where(dist >= n, dist - n, dist)
    dist = jnp.where(dist <= reach, dist, 0).astype(F32)
    far_row = jnp.max(dist, axis=0, keepdims=True)
    far = jnp.sum(jnp.where(ri == ci, far_row, 0.0), axis=1, keepdims=True)
    before = (far_row > far) | ((far_row == far) & (ci < ri))
    place = jnp.sum(jnp.where(before, 1.0, 0.0), axis=1, keepdims=True).astype(jnp.int32)
    lane = lax.rem(
        lax.broadcasted_iota(jnp.int32, (rows, BATCH * rows), 1),
        jnp.full((rows, BATCH * rows), rows, jnp.int32),
    )
    perm[...] = jnp.where(lane == place, 1.0, 0.0).astype(BF16)

    g = gate_ref[...]
    hi = g.astype(BF16).astype(F32)
    mid = (g - hi).astype(BF16).astype(F32)
    low = g - hi - mid
    for i, part in enumerate((ids.astype(F32), hi, mid, low)):
        meta_s[4 * i:4 * (i + 1), 0:LANES] = dot(part.astype(BF16), perm[:, 0:LANES])
    own[0:META, :] = meta_s[:, 0:LANES].astype(BF16)

    total = jnp.zeros((rows, CW), F32)
    for c in range(nch):
        v = tok_ref[:, c * CW:(c + 1) * CW].astype(F32)
        total = total + v * v
    scale = lax.rsqrt(jnp.sum(total, axis=1, keepdims=True) / width + epsilon)

    def ag_copy(src, k, c, count, to=ahead):
        first = 0 if c == 0 else META + rows * c
        span = pl.ds(first, META + rows * c + count - first)
        return pltpu.make_async_remote_copy(
            src_ref=src.at[span],
            dst_ref=ag.at[k, span],
            send_sem=ag_ss.at[k],
            recv_sem=got.at[k, c],
            device_id={"ep": to},
            device_id_type=MESH,
        )

    pl.semaphore_wait(barrier, 5)
    for c in range(nch):
        v = tok_ref[:, c * CW:(c + 1) * CW].astype(F32)
        normed = (v * scale * gain_ref[:, c * CW:(c + 1) * CW]).astype(BF16)
        sorted_rows = tdot(perm[:, 0:rows], normed).astype(BF16)
        for i in range(CW // LANES):
            at = c * (CW // LANES) + i
            own[META + rows * at:META + rows * (at + 1), :] = sorted_rows[:, i * LANES:(i + 1) * LANES]
            ag_copy(own, 1 - tp, at, rows).start()

    own_copy = pltpu.make_async_copy(own, ag.at[0], own_sem)

    @pl.when(tp == 0)
    def _():
        own_copy.start()

    for k in range(slots):
        if need(k) < rows:
            for c in range(fine):
                ag[k, META + rows * c + need(k):META + rows * (c + 1), :] = jnp.zeros(
                    (rows - need(k), LANES), BF16
                )

    bi = lax.broadcasted_iota(jnp.int32, (BATCH * rows, BATCH * rows), 0)
    bj = lax.broadcasted_iota(jnp.int32, (BATCH * rows, BATCH * rows), 1)
    upper[...] = jnp.where((bi // rows == bj // rows) & (bi < bj), 1.0, 0.0).astype(BF16)

    @pl.when(tp == 0)
    def _():
        own_copy.wait()

    half_cols = width // 2

    def x_copy(b, h):
        return pltpu.make_async_remote_copy(
            src_ref=x_own.at[b, h], dst_ref=x_sib.at[b, h], send_sem=x_ss.at[b, h],
            recv_sem=x_rs.at[b, h], device_id={"tp": sibling}, device_id_type=MESH,
        )

    def p_copy(b, h):
        return pltpu.make_async_remote_copy(
            src_ref=p_sib.at[b, h], dst_ref=p_rcv.at[b, h], send_sem=p_ss.at[b, h],
            recv_sem=p_rs.at[b, h], device_id={"tp": sibling}, device_id_type=MESH,
        )

    wide = BATCH * rows
    each = BATCH * cap

    def routing(b):
        per_tile = LANES // rows
        lane = lax.broadcasted_iota(jnp.int32, (META, LANES), 1) // rows
        for i in range(wide // LANES):
            mm = ag[b * BATCH + i * per_tile, 0:META, :].astype(F32)
            for j in range(1, per_tile):
                mm = jnp.where(lane == j, ag[b * BATCH + i * per_tile + j, 0:META, :].astype(F32), mm)
            meta_s[:, i * LANES:(i + 1) * LANES] = mm
        ids = [meta_s[k:k + 1, :] for k in range(4)]
        parts = [[meta_s[4 * (p + 1) + k:4 * (p + 1) + k + 1, :] for k in range(4)] for p in range(3)]
        row8 = lax.broadcasted_iota(jnp.int32, (8, wide), 0)
        members, gates = [], []
        for e in range(local):
            eid = (me * local + e).astype(F32)
            hits = [jnp.where(i == eid, 1.0, 0.0) for i in ids]
            members.append(sum(hits))
            gates.append([sum(h * g for h, g in zip(hits, part)) for part in parts])
        stacked = jnp.zeros((8, wide), F32)
        for e in range(local):
            stacked = jnp.where(row8 == e, members[e], stacked)
        rank_s[...] = dot(stacked.astype(BF16), upper[...])
        block = lax.broadcasted_iota(jnp.int32, (1, wide), 1) // rows
        row = lax.broadcasted_iota(jnp.int32, (each, wide), 0)
        for e in range(local):
            rank = rank_s[e:e + 1, :].astype(jnp.int32)
            key = jnp.where(members[e] > 0.5, block * cap + rank, -1)
            pick = jnp.where(row == key, 1.0, 0.0)
            sel[e * each:(e + 1) * each, :] = pick.astype(BF16)
            for p in range(3):
                at = (p * local + e) * each
                gsel[at:at + each, :] = (pick * gates[e][p]).astype(BF16)

    def select(b, c):
        block = jnp.concatenate([
            jnp.concatenate(
                [ag[b * BATCH + j, META + rows * at:META + rows * (at + 1), :] for j in range(BATCH)],
                axis=0,
            )
            for at in range(c * (CW // LANES), (c + 1) * (CW // LANES))
        ], axis=1)
        h, at = divmod(c, half_ch)
        x_own[b, h, :, at * CW:(at + 1) * CW] = dot(sel[...], block).astype(BF16)

    def expert_in(b, e, h):
        return jnp.concatenate(
            [x_own[b, h, e * each:(e + 1) * each, :], x_sib[b, h, e * each:(e + 1) * each, :]], axis=0
        )

    def gate_up(b, e):
        gate, up = 0.0, 0.0
        for h in range(2):
            x = expert_in(b, e, h)
            gate += dot(x, wg[e, h * half_cols:(h + 1) * half_cols, :])
            up += dot(x, wu[e, h * half_cols:(h + 1) * half_cols, :])
        hid[e] = (gate / (1.0 + jnp.exp(-gate)) * up).astype(BF16)

    def down(b, e, h):
        y = dot(hid[e], wd[e, :, h * half_cols:(h + 1) * half_cols]).astype(BF16)
        p_own[b, h, e * each:(e + 1) * each, :] = y[:each]
        p_sib[b, h, e * each:(e + 1) * each, :] = y[each:]

    def combine(b, c):
        h, at = divmod(c, half_ch)
        cols = slice(at * CW, (at + 1) * CW)
        y = (p_own[b, h, :, cols].astype(F32) + p_rcv[b, h, :, cols].astype(F32)).astype(BF16)
        g = tdot(gsel[...], jnp.concatenate([y, y, y], axis=0))
        for j in range(BATCH):
            contrib[b * BATCH + j, c] = g[j * rows:(j + 1) * rows]

    def run_all(*calls):
        def go():
            for call in calls:
                call()
        return go

    def pieces(b):
        call = functools.partial
        return {
            0: call(routing, b),
            1: run_all(*[call(select, b, c) for c in range(half_ch)], lambda: x_copy(b, 0).start()),
            2: run_all(*[call(select, b, c) for c in range(half_ch, nch)], lambda: x_copy(b, 1).start()),
            5: run_all(lambda: x_copy(b, 0).wait_recv(), lambda: x_copy(b, 1).wait_recv(), call(gate_up, b, 0)),
            6: call(down, b, 0, 0),
            7: call(down, b, 0, 1),
            8: call(gate_up, b, 1),
            9: run_all(call(down, b, 1, 0), lambda: p_copy(b, 0).start()),
            10: run_all(call(down, b, 1, 1), lambda: p_copy(b, 1).start()),
            14: run_all(lambda: p_copy(b, 0).wait_recv(), *[call(combine, b, c) for c in range(half_ch)]),
            15: run_all(lambda: p_copy(b, 1).wait_recv(), *[call(combine, b, c) for c in range(half_ch, nch)]),
        }

    def ag_step(b, j, c, final):
        k = b * BATCH + j

        def both(k, count, ahead_count):
            ag_copy(own, k, c, count).wait_recv()
            ag_copy(ag.at[k], k + 1, c, ahead_count).start()

        if final:
            k = last * BATCH + j
            if k < slots - 2:
                ag_copy(own, k, c, need(k)).wait_recv()
                if k == slots - 3:
                    ag_copy(ag.at[k], k + 2, c, need(k + 2), ahead2).start()
                ag_copy(ag.at[k], k + 1, c, need(k + 1)).start()
            else:
                ag_copy(own, k, c, need(k)).wait_recv()
        elif j == 0:
            pl.when(k + tp >= 1)(lambda: both(k, rows, rows))
        else:
            both(k, rows, rows)

    order = [(j, c) for j in range(BATCH) for c in range(fine)]
    per = len(order) // 16

    def window(b, _):
        work = pieces(b - 1)
        for i in range(16):
            for j, c in order[i * per:(i + 1) * per]:
                ag_step(b, j, c, False)
            if i in work:
                pl.when(b > 0)(work[i])
            if i == 4:
                @pl.when(b == 1)
                def _():
                    for copy in w_copies:
                        copy.wait()
        return 0

    lax.fori_loop(0, last, window, 0)

    work = pieces(last - 1)
    for i in range(16):
        for j, c in order[i * per:(i + 1) * per]:
            if j == BATCH - 1:
                continue
            ag_step(last, j, c, True)
        if i in work and i < 14:
            work[i]()
    work[14]()
    work[15]()

    for c in range(fine):
        ag_step(last, BATCH - 1, c, True)
        if c == 0:
            routing(last)
        done, odd = divmod(c + 1, CW // LANES)
        if odd == 0:
            select(last, done - 1)
            if done in (half_ch, nch):
                x_copy(last, done // half_ch - 1).start()
    partial = {}
    for h in range(2):
        x_copy(last, h).wait_recv()
        for e in range(local):
            x = expert_in(last, e, h)
            for i, w in enumerate((wg, wu)):
                y = dot(x, w[e, h * half_cols:(h + 1) * half_cols, :])
                partial[e, i] = y if h == 0 else partial[e, i] + y
    for e in range(local):
        gate, up = partial[e, 0], partial[e, 1]
        hid[e] = (gate / (1.0 + jnp.exp(-gate)) * up).astype(BF16)
    for h in range(2):
        for e in range(local):
            down(last, e, h)
        p_copy(last, h).start()

    def rs_copy(src, k, at, part):
        span = pl.ds(part[0], part[1] - part[0])
        return pltpu.make_async_remote_copy(
            src_ref=src.at[at, span],
            dst_ref=rs.at[k, at, span],
            send_sem=rs_ss.at[k],
            recv_sem=got.at[k, at * 2 + part[0] // split],
            device_id={"ep": behind},
            device_id_type=MESH,
        )

    def skip_copy(c):
        span = pl.ds(0, need(slots - 1))
        return pltpu.make_async_remote_copy(
            src_ref=rs0.at[c, span],
            dst_ref=skip.at[c],
            send_sem=rs_ss.at[slots - 1],
            recv_sem=got.at[slots + 1, c],
            device_id={"ep": behind2},
            device_id_type=MESH,
        )

    def turn(c):
        at = c + sibling * half_ch
        return jnp.where(at >= nch, at - nch, at)

    for h in range(2):
        p_copy(last, h).wait_recv()
        for c in range(h * half_ch, (h + 1) * half_ch):
            combine(last, c)
            rs0[c, 0:need(slots - 1), :] = contrib[slots - 1, c, 0:need(slots - 1), :].astype(BF16)
            skip_copy(c).start()
            k, count = slots - 2, need(slots - 2)
            rs[k, c, 0:count, :] = contrib[k, c, 0:count, :].astype(BF16)
            for part in parts(count):
                rs_copy(rs.at[k], k - 1, c, part).start()

    def rs_add(k, to, at, there, count, skipped=0):
        for lo, hi in parts(count):
            mid = max(lo, min(hi, there))
            if lo < mid:
                rs_copy(rs0, k, at, (lo, mid)).wait_recv()
                if lo < skipped:
                    skip_copy(at).wait_recv()
                    contrib[k, at, lo:skipped, :] += skip[at].astype(F32)
                rs[k, at, lo:mid, :] = (
                    rs[k, at, lo:mid, :].astype(F32) + contrib[k, at, lo:mid, :]
                ).astype(BF16)
            if mid < hi:
                rs[k, at, mid:hi, :] = contrib[k, at, mid:hi, :].astype(BF16)
            rs_copy(rs.at[k], to, at, (lo, hi)).start()

    def rs_step(k, there, count, skipped=0):
        for c in range(nch):
            rs_add(k, k - 1, turn(c), there, count, skipped)

    k = slots - 3
    rs_step(k, need(k + 1), need(k), need(slots - 1))
    k -= 1
    while need(k + 1) < rows:
        rs_step(k, need(k + 1), need(k))
        k -= 1
    top_k = k

    def rs_loop(i, _):
        rs_step(top_k - i, rows, rows)
        return 0

    lax.fori_loop(0, top_k, rs_loop, 0)

    @pl.when(tp == 1)
    def _():
        for c in range(nch):
            rs_add(0, slots, turn(c), rows, rows)
    def ag_sent(k, count):
        size = pl.ds(0, META + fine * count)
        pltpu.make_async_remote_copy(
            src_ref=ag.at[k, size], dst_ref=ag.at[k, size], send_sem=ag_ss.at[k],
            recv_sem=got.at[k, 0], device_id={"ep": ahead}, device_id_type=MESH,
        ).wait_send()

    def rs_sent(k, count):
        size = pl.ds(0, count)
        pltpu.make_async_remote_copy(
            src_ref=rs.at[k, :, size], dst_ref=rs.at[k, :, size], send_sem=rs_ss.at[k],
            recv_sem=got.at[k, 0], device_id={"ep": behind}, device_id_type=MESH,
        ).wait_send()

    pl.when(tp == 1)(functools.partial(ag_sent, 0, rows))
    for k in range(1, slots):
        ag_sent(k, need(k))
    for b in range(batches):
        for h in range(2):
            x_copy(b, h).wait_send()
            p_copy(b, h).wait_send()
    for k in range(3, slots - 2):
        rs_sent(k, need(k + 1))

    end = jnp.where(tp == 1, slots, 0)
    share = (1 - tp).astype(F32)

    def f_copy(c):
        return pltpu.make_async_remote_copy(
            src_ref=rs0.at[c], dst_ref=fin.at[c], send_sem=f_ss.at[c],
            recv_sem=f_rs.at[c], device_id={"tp": sibling}, device_id_type=MESH,
        )

    size = pl.ds(0, need(slots - 1))
    pltpu.make_async_remote_copy(
        src_ref=rs0.at[:, size], dst_ref=rs0.at[:, size], send_sem=rs_ss.at[slots - 1],
        recv_sem=got.at[slots - 1, 0], device_id={"ep": behind2}, device_id_type=MESH,
    ).wait_send()
    for c in range(nch):
        at = turn(c)
        for part in parts(rows):
            rs_copy(rs0, end, at, part).wait_recv()
        v = (rs[end, at].astype(F32) + share * contrib[0, at]).astype(BF16)
        y = dot(perm[:, 0:rows], v)
        if c < half_ch:
            rs0[c] = y.astype(BF16)
            f_copy(c).start()
        else:
            i = c - half_ch
            f_copy(i).wait_recv()
            out_ref[:, i * CW:(i + 1) * CW] = (y + fin[i].astype(F32)).astype(BF16)

    for k in range(3):
        rs_sent(k, need(k + 1))

    @pl.when(tp == 1)
    def _():
        rs_sent(slots, rows)

    for c in range(half_ch):
        f_copy(c).wait_send()


def on_device(tokens, norm_gain, groups, picks, gates, w_gate, w_up, w_down):
    rows, width = tokens.shape
    top = picks.shape[1]
    local, _, ffl = w_gate.shape
    n = lax.axis_size("ep")
    group_experts = n * local // GROUPS
    cap = rows * top // group_experts
    slots = n // 2
    batches = slots // BATCH
    nch = width // CW
    batch_rows = local * BATCH * cap
    vmem = pltpu.VMEM
    dma = pltpu.SemaphoreType.DMA
    return pl.pallas_call(
        functools.partial(kernel, n, rows, width, local, cap, group_experts),
        out_shape=pltpu.VMEM((rows, width // 2), BF16),
        in_specs=[pl.BlockSpec(memory_space=pltpu.VMEM)] * 5 + [pl.BlockSpec(memory_space=pl.ANY)] * 3,
        out_specs=pl.BlockSpec(memory_space=pltpu.VMEM),
        scratch_shapes=[
            vmem((META + rows * width // LANES, LANES), BF16),
            vmem((slots, META + rows * width // LANES, LANES), BF16),
            vmem((slots + 1, nch, rows, CW), BF16),
            vmem((nch, rows, CW), BF16),
            vmem((slots, nch, rows, CW), F32),
            vmem(w_gate.shape, BF16),
            vmem(w_up.shape, BF16),
            vmem(w_down.shape, BF16),
            vmem((batches, 2, batch_rows, width // 2), BF16),
            vmem((batches, 2, batch_rows, width // 2), BF16),
            vmem((batches, 2, batch_rows, width // 2), BF16),
            vmem((batches, 2, batch_rows, width // 2), BF16),
            vmem((batches, 2, batch_rows, width // 2), BF16),
            vmem((nch // 2, rows, CW), BF16),
            vmem((batch_rows, BATCH * rows), BF16),
            vmem((3 * batch_rows, BATCH * rows), BF16),
            vmem((META, BATCH * rows), F32),
            vmem((8, BATCH * rows), F32),
            vmem((BATCH * rows, BATCH * rows), BF16),
            vmem((local, 2 * BATCH * cap, ffl), BF16),
            vmem((rows, BATCH * rows), BF16),
            vmem((nch, local * cap, CW), BF16),
            dma((slots,)), dma((slots + 2, width // LANES)), dma((slots + 1,)),
            dma((batches, 2)), dma((batches, 2)), dma((batches, 2)), dma((batches, 2)),
            dma((nch // 2,)), dma((nch // 2,)), dma((3,)), dma,
        ],
        compiler_params=pltpu.CompilerParams(
            collective_id=0, has_side_effects=True, vmem_limit_bytes=60 * 2**20
        ),
    )(
        tokens, norm_gain.reshape(1, width), groups.reshape(1, rows), picks.T, gates.T,
        w_gate, w_up, w_down,
    )


def solution(mesh):
    in_specs = (
        P(("grp", "ep"), None),
        P(),
        P(("grp", "ep")),
        P(("grp", "ep"), None),
        P(("grp", "ep"), None),
        P("ep", None, "tp"),
        P("ep", None, "tp"),
        P("ep", "tp", None),
    )
    out_specs = P(("grp", "ep"), "tp")
    return jax.shard_map(
        on_device, mesh=mesh, in_specs=in_specs, out_specs=out_specs, check_vma=False
    )
```

```python
import functools

import jax
import jax.numpy as jnp
from jax import lax
from jax.experimental import pallas as pl
from jax.experimental.pallas import tpu as pltpu
from jax.sharding import PartitionSpec as P

GROUPS = 2
MESH = pl.DeviceIdType.MESH
F32 = jnp.float32
BF16 = jnp.bfloat16
CW = 256
LANES = 128
META = 16
BATCH = 4

epsilon = 1e-06


def dot(a, b):
    return jnp.dot(a, b, preferred_element_type=F32)


def tdot(a, b):
    return lax.dot_general(a, b, (((0,), (0,)), ((), ())), preferred_element_type=F32)


def kernel(
    n, rows, width, local, cap, group_experts,
    tok_ref, gain_ref, grp_ref, pick_ref, gate_ref, wg_hbm, wu_hbm, wd_hbm, out_ref,
    own, ag, rs, rs0, contrib, wg, wu, wd, x_own, x_sib, p_own, p_sib, p_rcv, fin,
    sel, gsel, meta_s, rank_s, upper, hid, perm, skip, acc,
    ag_ss, got, rs_ss, x_ss, x_rs, p_ss, p_rs, f_ss, f_rs, w_sem, own_sem,
):
    slots = n // 2
    batches = slots // BATCH
    last = batches - 1
    nch = width // CW
    half_ch = nch // 2
    fine = width // LANES
    me = lax.axis_index("ep")
    tp = lax.axis_index("tp")
    right, left = lax.rem(me + 1, n), lax.rem(me + n - 1, n)
    ahead = jnp.where(tp == 1, right, left)
    behind = jnp.where(tp == 1, left, right)
    ahead2 = lax.rem(ahead + ahead - me + n, n)
    behind2 = lax.rem(behind + behind - me + n, n)
    reach = slots - 1 + tp
    sibling = 1 - tp

    barrier = pltpu.get_barrier_semaphore()
    for peer in (ahead2, behind2, ahead, behind):
        pl.semaphore_signal(barrier, inc=1, device_id={"ep": peer}, device_id_type=MESH)
    pl.semaphore_signal(barrier, inc=1, device_id={"tp": sibling}, device_id_type=MESH)

    w_copies = [
        pltpu.make_async_copy(src, dst, w_sem.at[i])
        for i, (src, dst) in enumerate(((wg_hbm, wg), (wu_hbm, wu), (wd_hbm, wd)))
    ]
    for copy in w_copies:
        copy.start()

    split = rows // 2

    def parts(count):
        return [(lo, min(count, lo + split)) for lo in range(0, count, split)]

    def need(k):
        return min(rows, local * cap * (slots - k))

    ri = lax.broadcasted_iota(jnp.int32, (rows, rows), 0)
    ci = lax.broadcasted_iota(jnp.int32, (rows, rows), 1)
    ids = grp_ref[...] * group_experts + pick_ref[...]
    chip = lax.div(ids, jnp.full(ids.shape, local, jnp.int32))
    dist = (chip - me) * (2 * tp - 1) + n
    dist = jnp.where(dist >= n, dist - n, dist)
    dist = jnp.where(dist <= reach, dist, 0).astype(F32)
    far_row = jnp.max(dist, axis=0, keepdims=True)
    far = jnp.sum(jnp.where(ri == ci, far_row, 0.0), axis=1, keepdims=True)
    before = (far_row > far) | ((far_row == far) & (ci < ri))
    place = jnp.sum(jnp.where(before, 1.0, 0.0), axis=1, keepdims=True).astype(jnp.int32)
    lane = lax.rem(
        lax.broadcasted_iota(jnp.int32, (rows, BATCH * rows), 1),
        jnp.full((rows, BATCH * rows), rows, jnp.int32),
    )
    perm[...] = jnp.where(lane == place, 1.0, 0.0).astype(BF16)

    g = gate_ref[...]
    hi = g.astype(BF16).astype(F32)
    mid = (g - hi).astype(BF16).astype(F32)
    low = g - hi - mid
    for i, part in enumerate((ids.astype(F32), hi, mid, low)):
        meta_s[4 * i:4 * (i + 1), 0:LANES] = dot(part.astype(BF16), perm[:, 0:LANES])
    own[0:META, :] = meta_s[:, 0:LANES].astype(BF16)

    total = jnp.zeros((rows, CW), F32)
    for c in range(nch):
        v = tok_ref[:, c * CW:(c + 1) * CW].astype(F32)
        total = total + v * v
    scale = lax.rsqrt(jnp.sum(total, axis=1, keepdims=True) / width + epsilon)

    def ag_copy(src, k, c, count, to=ahead):
        first = 0 if c == 0 else META + rows * c
        span = pl.ds(first, META + rows * c + count - first)
        return pltpu.make_async_remote_copy(
            src_ref=src.at[span],
            dst_ref=ag.at[k, span],
            send_sem=ag_ss.at[k],
            recv_sem=got.at[k, c],
            device_id={"ep": to},
            device_id_type=MESH,
        )

    pl.semaphore_wait(barrier, 5)
    for c in range(nch):
        v = tok_ref[:, c * CW:(c + 1) * CW].astype(F32)
        normed = (v * scale * gain_ref[:, c * CW:(c + 1) * CW]).astype(BF16)
        sorted_rows = tdot(perm[:, 0:rows], normed).astype(BF16)
        for i in range(CW // LANES):
            at = c * (CW // LANES) + i
            own[META + rows * at:META + rows * (at + 1), :] = sorted_rows[:, i * LANES:(i + 1) * LANES]
            ag_copy(own, 1 - tp, at, rows).start()

    own_copy = pltpu.make_async_copy(own, ag.at[0], own_sem)

    @pl.when(tp == 0)
    def _():
        own_copy.start()

    for k in range(slots):
        if need(k) < rows:
            for c in range(fine):
                ag[k, META + rows * c + need(k):META + rows * (c + 1), :] = jnp.zeros(
                    (rows - need(k), LANES), BF16
                )

    bi = lax.broadcasted_iota(jnp.int32, (BATCH * rows, BATCH * rows), 0)
    bj = lax.broadcasted_iota(jnp.int32, (BATCH * rows, BATCH * rows), 1)
    upper[...] = jnp.where((bi // rows == bj // rows) & (bi < bj), 1.0, 0.0).astype(BF16)

    @pl.when(tp == 0)
    def _():
        own_copy.wait()

    half_cols = width // 2

    def x_copy(b, h):
        return pltpu.make_async_remote_copy(
            src_ref=x_own.at[b, h], dst_ref=x_sib.at[b, h], send_sem=x_ss.at[b, h],
            recv_sem=x_rs.at[b, h], device_id={"tp": sibling}, device_id_type=MESH,
        )

    def p_copy(b, h):
        return pltpu.make_async_remote_copy(
            src_ref=p_sib.at[b, h], dst_ref=p_rcv.at[b, h], send_sem=p_ss.at[b, h],
            recv_sem=p_rs.at[b, h], device_id={"tp": sibling}, device_id_type=MESH,
        )

    wide = BATCH * rows
    each = BATCH * cap

    def routing(b):
        per_tile = LANES // rows
        lane = lax.broadcasted_iota(jnp.int32, (META, LANES), 1) // rows
        for i in range(wide // LANES):
            mm = ag[b * BATCH + i * per_tile, 0:META, :].astype(F32)
            for j in range(1, per_tile):
                mm = jnp.where(lane == j, ag[b * BATCH + i * per_tile + j, 0:META, :].astype(F32), mm)
            meta_s[:, i * LANES:(i + 1) * LANES] = mm
        ids = [meta_s[k:k + 1, :] for k in range(4)]
        parts = [[meta_s[4 * (p + 1) + k:4 * (p + 1) + k + 1, :] for k in range(4)] for p in range(3)]
        row8 = lax.broadcasted_iota(jnp.int32, (8, wide), 0)
        members, gates = [], []
        for e in range(local):
            eid = (me * local + e).astype(F32)
            hits = [jnp.where(i == eid, 1.0, 0.0) for i in ids]
            members.append(sum(hits))
            gates.append([sum(h * g for h, g in zip(hits, part)) for part in parts])
        stacked = jnp.zeros((8, wide), F32)
        for e in range(local):
            stacked = jnp.where(row8 == e, members[e], stacked)
        rank_s[...] = dot(stacked.astype(BF16), upper[...])
        block = lax.broadcasted_iota(jnp.int32, (1, wide), 1) // rows
        row = lax.broadcasted_iota(jnp.int32, (each, wide), 0)
        for e in range(local):
            rank = rank_s[e:e + 1, :].astype(jnp.int32)
            key = jnp.where(members[e] > 0.5, block * cap + rank, -1)
            pick = jnp.where(row == key, 1.0, 0.0)
            sel[e * each:(e + 1) * each, :] = pick.astype(BF16)
            for p in range(3):
                at = (p * local + e) * each
                gsel[at:at + each, :] = (pick * gates[e][p]).astype(BF16)

    def select(b, c):
        block = jnp.concatenate([
            jnp.concatenate(
                [ag[b * BATCH + j, META + rows * at:META + rows * (at + 1), :] for j in range(BATCH)],
                axis=0,
            )
            for at in range(c * (CW // LANES), (c + 1) * (CW // LANES))
        ], axis=1)
        h, at = divmod(c, half_ch)
        x_own[b, h, :, at * CW:(at + 1) * CW] = dot(sel[...], block).astype(BF16)

    def expert_in(b, e, h):
        return jnp.concatenate(
            [x_own[b, h, e * each:(e + 1) * each, :], x_sib[b, h, e * each:(e + 1) * each, :]], axis=0
        )

    def half(h):
        return pl.ds(pl.multiple_of(h * half_cols, half_cols), half_cols)

    def activate(e, gate, up):
        hid[e] = (gate / (1.0 + jnp.exp(-gate)) * up).astype(BF16)

    def gate_up(b, e, h):
        x = expert_in(b, e, h)
        gate = dot(x, wg[e, h * half_cols:(h + 1) * half_cols, :])
        up = dot(x, wu[e, h * half_cols:(h + 1) * half_cols, :])
        if h == 0:
            acc[0], acc[1] = gate, up
        else:
            activate(e, acc[0] + gate, acc[1] + up)

    def down(b, e, h):
        y = dot(hid[e], wd[e, :, h * half_cols:(h + 1) * half_cols]).astype(BF16)
        p_own[b, h, e * each:(e + 1) * each, :] = y[:each]
        p_sib[b, h, e * each:(e + 1) * each, :] = y[each:]

    def combine(b, h, at):
        cols = slice(at * CW, (at + 1) * CW)
        y = (p_own[b, h, :, cols].astype(F32) + p_rcv[b, h, :, cols].astype(F32)).astype(BF16)
        g = tdot(gsel[...], jnp.concatenate([y, y, y], axis=0))
        for j in range(BATCH):
            contrib[b * BATCH + j, h * half_ch + at] = g[j * rows:(j + 1) * rows]

    def pieces(b):
        call = functools.partial
        work = {0: [call(routing, b)]}
        for c in range(nch):
            work[1 + c] = [call(select, b, c)]
        for h in range(2):
            work[(h + 1) * half_ch].append(lambda h=h: x_copy(b, h).start())
            work[12 + h] = [lambda h=h: x_copy(b, h).wait_recv(), call(gate_up, b, 0, h)]
            work[14 + h] = [call(down, b, 0, h)]
            work[16 + h] = [call(gate_up, b, 1, h)]
            work[18 + h] = [call(down, b, 1, h), lambda h=h: p_copy(b, h).start()]
            for at in range(half_ch):
                work[24 + h * half_ch + at] = [call(combine, b, h, at)]
            work[24 + h * half_ch].insert(0, lambda h=h: p_copy(b, h).wait_recv())

        def joined(calls):
            def go():
                for each_call in calls:
                    each_call()
            return go

        return {at: joined(calls) for at, calls in work.items()}

    def ag_step(b, j, c, final):
        k = b * BATCH + j

        def both(k, count, ahead_count):
            ag_copy(own, k, c, count).wait_recv()
            ag_copy(ag.at[k], k + 1, c, ahead_count).start()

        if final:
            k = last * BATCH + j
            if k < slots - 2:
                ag_copy(own, k, c, need(k)).wait_recv()
                if k == slots - 3:
                    ag_copy(ag.at[k], k + 2, c, need(k + 2), ahead2).start()
                ag_copy(ag.at[k], k + 1, c, need(k + 1)).start()
            else:
                ag_copy(own, k, c, need(k)).wait_recv()
        elif j == 0:
            pl.when(k + tp >= 1)(lambda: both(k, rows, rows))
        else:
            both(k, rows, rows)

    order = [(j, c) for j in range(BATCH) for c in range(fine)]
    places = 32
    per = len(order) // places

    def window(b, _):
        work = pieces(b - 1)
        for i in range(places):
            for j, c in order[i * per:(i + 1) * per]:
                ag_step(b, j, c, False)
            if i in work:
                pl.when(b > 0)(work[i])
            if i == 10:
                @pl.when(b == 1)
                def _():
                    for copy in w_copies:
                        copy.wait()
        return 0

    lax.fori_loop(0, last, window, 0)

    work = pieces(last - 1)
    lead = [(j, c) for j, c in order if j < BATCH - 1]
    for i in range(places):
        for j, c in lead[i * len(lead) // places:(i + 1) * len(lead) // places]:
            ag_step(last, j, c, True)
        if i in work:
            work[i]()

    for c in range(fine):
        ag_step(last, BATCH - 1, c, True)
        if c == 0:
            routing(last)
        done, odd = divmod(c + 1, CW // LANES)
        if odd == 0:
            select(last, done - 1)
            if done in (half_ch, nch):
                x_copy(last, done // half_ch - 1).start()
    partial = {}
    for h in range(2):
        x_copy(last, h).wait_recv()
        for e in range(local):
            x = expert_in(last, e, h)
            for i, w in enumerate((wg, wu)):
                y = dot(x, w[e, h * half_cols:(h + 1) * half_cols, :])
                partial[e, i] = y if h == 0 else partial[e, i] + y
    for e in range(local):
        activate(e, partial[e, 0], partial[e, 1])
    for mine, theirs in ((sibling, tp), (tp, sibling)):
        for e in range(local):
            y = dot(hid[e, each:2 * each, :], wd[e, :, half(theirs)])
            p_sib[last, theirs, e * each:(e + 1) * each, :] = y.astype(BF16)
        p_copy(last, theirs).start()
        for e in range(local):
            y = dot(hid[e, 0:each, :], wd[e, :, half(mine)])
            p_own[last, mine, e * each:(e + 1) * each, :] = y.astype(BF16)

    def rs_copy(src, k, at, part):
        span = pl.ds(part[0], part[1] - part[0])
        return pltpu.make_async_remote_copy(
            src_ref=src.at[at, span],
            dst_ref=rs.at[k, at, span],
            send_sem=rs_ss.at[k],
            recv_sem=got.at[k, at * 2 + part[0] // split],
            device_id={"ep": behind},
            device_id_type=MESH,
        )

    def skip_copy(c):
        span = pl.ds(0, need(slots - 1))
        return pltpu.make_async_remote_copy(
            src_ref=rs0.at[c, span],
            dst_ref=skip.at[c],
            send_sem=rs_ss.at[slots - 1],
            recv_sem=got.at[slots + 1, c],
            device_id={"ep": behind2},
            device_id_type=MESH,
        )

    def turn(c):
        at = c + sibling * half_ch
        return jnp.where(at >= nch, at - nch, at)

    for h in (sibling, tp):
        p_copy(last, h).wait_recv()
        for at in range(half_ch):
            combine(last, h, at)
            c = h * half_ch + at
            count = need(slots - 1)
            rs0[c, 0:count, :] = contrib[slots - 1, c, 0:count, :].astype(BF16)
            skip_copy(c).start()
            k, count = slots - 2, need(slots - 2)
            rs[k, c, 0:count, :] = contrib[k, c, 0:count, :].astype(BF16)
            for part in parts(count):
                rs_copy(rs.at[k], k - 1, c, part).start()

    def rs_add(k, to, at, there, count, skipped=0):
        for lo, hi in parts(count):
            mid = max(lo, min(hi, there))
            if lo < mid:
                rs_copy(rs0, k, at, (lo, mid)).wait_recv()
                if lo < skipped:
                    skip_copy(at).wait_recv()
                    contrib[k, at, lo:skipped, :] += skip[at].astype(F32)
                rs[k, at, lo:mid, :] = (
                    rs[k, at, lo:mid, :].astype(F32) + contrib[k, at, lo:mid, :]
                ).astype(BF16)
            if mid < hi:
                rs[k, at, mid:hi, :] = contrib[k, at, mid:hi, :].astype(BF16)
            rs_copy(rs.at[k], to, at, (lo, hi)).start()

    def rs_step(k, there, count, skipped=0):
        for c in range(nch):
            rs_add(k, k - 1, turn(c), there, count, skipped)

    k = slots - 3
    rs_step(k, need(k + 1), need(k), need(slots - 1))
    k -= 1
    while need(k + 1) < rows:
        rs_step(k, need(k + 1), need(k))
        k -= 1
    top_k = k

    def rs_loop(i, _):
        rs_step(top_k - i, rows, rows)
        return 0

    lax.fori_loop(0, top_k, rs_loop, 0)

    @pl.when(tp == 1)
    def _():
        for c in range(nch):
            rs_add(0, slots, turn(c), rows, rows)
    def ag_sent(k, count):
        size = pl.ds(0, META + fine * count)
        pltpu.make_async_remote_copy(
            src_ref=ag.at[k, size], dst_ref=ag.at[k, size], send_sem=ag_ss.at[k],
            recv_sem=got.at[k, 0], device_id={"ep": ahead}, device_id_type=MESH,
        ).wait_send()

    def rs_sent(k, count):
        size = pl.ds(0, count)
        pltpu.make_async_remote_copy(
            src_ref=rs.at[k, :, size], dst_ref=rs.at[k, :, size], send_sem=rs_ss.at[k],
            recv_sem=got.at[k, 0], device_id={"ep": behind}, device_id_type=MESH,
        ).wait_send()

    pl.when(tp == 1)(functools.partial(ag_sent, 0, rows))
    for k in range(1, slots):
        ag_sent(k, need(k))
    for b in range(batches):
        for h in range(2):
            x_copy(b, h).wait_send()
            p_copy(b, h).wait_send()
    for k in range(3, slots - 2):
        rs_sent(k, need(k + 1))

    end = jnp.where(tp == 1, slots, 0)
    share = (1 - tp).astype(F32)

    def f_copy(c):
        return pltpu.make_async_remote_copy(
            src_ref=rs0.at[c], dst_ref=fin.at[c], send_sem=f_ss.at[c],
            recv_sem=f_rs.at[c], device_id={"tp": sibling}, device_id_type=MESH,
        )

    size = pl.ds(0, need(slots - 1))
    pltpu.make_async_remote_copy(
        src_ref=rs0.at[:, size], dst_ref=rs0.at[:, size], send_sem=rs_ss.at[slots - 1],
        recv_sem=got.at[slots - 1, 0], device_id={"ep": behind2}, device_id_type=MESH,
    ).wait_send()
    for c in range(nch):
        at = turn(c)
        for part in parts(rows):
            rs_copy(rs0, end, at, part).wait_recv()
        v = (rs[end, at].astype(F32) + share * contrib[0, at]).astype(BF16)
        y = dot(perm[:, 0:rows], v)
        if c < half_ch:
            rs0[c] = y.astype(BF16)
            f_copy(c).start()
        else:
            i = c - half_ch
            f_copy(i).wait_recv()
            out_ref[:, i * CW:(i + 1) * CW] = (y + fin[i].astype(F32)).astype(BF16)

    for k in range(3):
        rs_sent(k, need(k + 1))

    @pl.when(tp == 1)
    def _():
        rs_sent(slots, rows)

    for c in range(half_ch):
        f_copy(c).wait_send()


def on_device(tokens, norm_gain, groups, picks, gates, w_gate, w_up, w_down):
    rows, width = tokens.shape
    top = picks.shape[1]
    local, _, ffl = w_gate.shape
    n = lax.axis_size("ep")
    group_experts = n * local // GROUPS
    cap = rows * top // group_experts
    slots = n // 2
    batches = slots // BATCH
    nch = width // CW
    batch_rows = local * BATCH * cap
    vmem = pltpu.VMEM
    dma = pltpu.SemaphoreType.DMA
    return pl.pallas_call(
        functools.partial(kernel, n, rows, width, local, cap, group_experts),
        out_shape=pltpu.VMEM((rows, width // 2), BF16),
        in_specs=[pl.BlockSpec(memory_space=pltpu.VMEM)] * 5 + [pl.BlockSpec(memory_space=pl.ANY)] * 3,
        out_specs=pl.BlockSpec(memory_space=pltpu.VMEM),
        scratch_shapes=[
            vmem((META + rows * width // LANES, LANES), BF16),
            vmem((slots, META + rows * width // LANES, LANES), BF16),
            vmem((slots + 1, nch, rows, CW), BF16),
            vmem((nch, rows, CW), BF16),
            vmem((slots, nch, rows, CW), F32),
            vmem(w_gate.shape, BF16),
            vmem(w_up.shape, BF16),
            vmem(w_down.shape, BF16),
            vmem((batches, 2, batch_rows, width // 2), BF16),
            vmem((batches, 2, batch_rows, width // 2), BF16),
            vmem((batches, 2, batch_rows, width // 2), BF16),
            vmem((batches, 2, batch_rows, width // 2), BF16),
            vmem((batches, 2, batch_rows, width // 2), BF16),
            vmem((nch // 2, rows, CW), BF16),
            vmem((batch_rows, BATCH * rows), BF16),
            vmem((3 * batch_rows, BATCH * rows), BF16),
            vmem((META, BATCH * rows), F32),
            vmem((8, BATCH * rows), F32),
            vmem((BATCH * rows, BATCH * rows), BF16),
            vmem((local, 2 * BATCH * cap, ffl), BF16),
            vmem((rows, BATCH * rows), BF16),
            vmem((nch, local * cap, CW), BF16),
            vmem((2, 2 * BATCH * cap, ffl), F32),
            dma((slots,)), dma((slots + 2, width // LANES)), dma((slots + 1,)),
            dma((batches, 2)), dma((batches, 2)), dma((batches, 2)), dma((batches, 2)),
            dma((nch // 2,)), dma((nch // 2,)), dma((3,)), dma,
        ],
        compiler_params=pltpu.CompilerParams(
            collective_id=0, has_side_effects=True, vmem_limit_bytes=60 * 2**20
        ),
    )(
        tokens, norm_gain.reshape(1, width), groups.reshape(1, rows), picks.T, gates.T,
        w_gate, w_up, w_down,
    )


def solution(mesh):
    in_specs = (
        P(("grp", "ep"), None),
        P(),
        P(("grp", "ep")),
        P(("grp", "ep"), None),
        P(("grp", "ep"), None),
        P("ep", None, "tp"),
        P("ep", None, "tp"),
        P("ep", "tp", None),
    )
    out_specs = P(("grp", "ep"), "tp")
    return jax.shard_map(
        on_device, mesh=mesh, in_specs=in_specs, out_specs=out_specs, check_vma=False
    )
```

```python
import functools

import jax
import jax.numpy as jnp
from jax import lax
from jax.experimental import pallas as pl
from jax.experimental.pallas import tpu as pltpu
from jax.sharding import PartitionSpec as P

GROUPS = 2
MESH = pl.DeviceIdType.MESH
F32 = jnp.float32
BF16 = jnp.bfloat16
CW = 256
LANES = 128
META = 16
BATCH = 4

epsilon = 1e-06


def dot(a, b):
    return jnp.dot(a, b, preferred_element_type=F32)


def tdot(a, b):
    return lax.dot_general(a, b, (((0,), (0,)), ((), ())), preferred_element_type=F32)


def kernel(
    n, rows, width, local, cap, group_experts,
    tok_ref, gain_ref, grp_ref, pick_ref, gate_ref, wg_hbm, wu_hbm, wd_hbm, out_ref,
    own, ag, rs, rs0, contrib, wg, wu, wd, x_own, x_sib, p_own, p_sib, p_rcv, fin,
    sel, gsel, meta_s, rank_s, upper, hid, perm, skip, acc,
    ag_ss, got, rs_ss, x_ss, x_rs, p_ss, p_rs, f_ss, f_rs, w_sem, own_sem,
):
    slots = n // 2
    batches = slots // BATCH
    last = batches - 1
    nch = width // CW
    half_ch = nch // 2
    fine = width // LANES
    me = lax.axis_index("ep")
    tp = lax.axis_index("tp")
    right, left = lax.rem(me + 1, n), lax.rem(me + n - 1, n)
    ahead = jnp.where(tp == 1, right, left)
    behind = jnp.where(tp == 1, left, right)
    ahead2 = lax.rem(ahead + ahead - me + n, n)
    behind2 = lax.rem(behind + behind - me + n, n)
    reach = slots - 1 + tp
    sibling = 1 - tp

    barrier = pltpu.get_barrier_semaphore()
    for peer in (ahead2, behind2, ahead, behind):
        pl.semaphore_signal(barrier, inc=1, device_id={"ep": peer}, device_id_type=MESH)
    pl.semaphore_signal(barrier, inc=1, device_id={"tp": sibling}, device_id_type=MESH)

    w_copies = [
        pltpu.make_async_copy(src, dst, w_sem.at[i])
        for i, (src, dst) in enumerate(((wg_hbm, wg), (wu_hbm, wu), (wd_hbm, wd)))
    ]
    for copy in w_copies:
        copy.start()

    split = rows // 2

    def parts(count):
        return [(lo, min(count, lo + split)) for lo in range(0, count, split)]

    def need(k):
        return min(rows, local * cap * (slots - k))

    ri = lax.broadcasted_iota(jnp.int32, (rows, rows), 0)
    ci = lax.broadcasted_iota(jnp.int32, (rows, rows), 1)
    ids = grp_ref[...] * group_experts + pick_ref[...]
    chip = lax.div(ids, jnp.full(ids.shape, local, jnp.int32))
    dist = (chip - me) * (2 * tp - 1) + n
    dist = jnp.where(dist >= n, dist - n, dist)
    dist = jnp.where(dist <= reach, dist, 0).astype(F32)
    far_row = jnp.max(dist, axis=0, keepdims=True)
    far = jnp.sum(jnp.where(ri == ci, far_row, 0.0), axis=1, keepdims=True)
    before = (far_row > far) | ((far_row == far) & (ci < ri))
    place = jnp.sum(jnp.where(before, 1.0, 0.0), axis=1, keepdims=True).astype(jnp.int32)
    lane = lax.rem(
        lax.broadcasted_iota(jnp.int32, (rows, BATCH * rows), 1),
        jnp.full((rows, BATCH * rows), rows, jnp.int32),
    )
    perm[...] = jnp.where(lane == place, 1.0, 0.0).astype(BF16)

    g = gate_ref[...]
    hi = g.astype(BF16).astype(F32)
    mid = (g - hi).astype(BF16).astype(F32)
    low = g - hi - mid
    for i, part in enumerate((ids.astype(F32), hi, mid, low)):
        meta_s[4 * i:4 * (i + 1), 0:LANES] = dot(part.astype(BF16), perm[:, 0:LANES])
    own[0:META, :] = meta_s[:, 0:LANES].astype(BF16)

    total = jnp.zeros((rows, CW), F32)
    for c in range(nch):
        v = tok_ref[:, c * CW:(c + 1) * CW].astype(F32)
        total = total + v * v
    scale = lax.rsqrt(jnp.sum(total, axis=1, keepdims=True) / width + epsilon)

    def ag_copy(src, k, c, count, to=ahead):
        first = 0 if c == 0 else META + rows * c
        span = pl.ds(first, META + rows * c + count - first)
        return pltpu.make_async_remote_copy(
            src_ref=src.at[span],
            dst_ref=ag.at[k, span],
            send_sem=ag_ss.at[k],
            recv_sem=got.at[k, c],
            device_id={"ep": to},
            device_id_type=MESH,
        )

    pl.semaphore_wait(barrier, 5)
    for c in range(nch):
        v = tok_ref[:, c * CW:(c + 1) * CW].astype(F32)
        normed = (v * scale * gain_ref[:, c * CW:(c + 1) * CW]).astype(BF16)
        sorted_rows = tdot(perm[:, 0:rows], normed).astype(BF16)
        for i in range(CW // LANES):
            at = c * (CW // LANES) + i
            own[META + rows * at:META + rows * (at + 1), :] = sorted_rows[:, i * LANES:(i + 1) * LANES]
            ag_copy(own, 1 - tp, at, rows).start()

    own_copy = pltpu.make_async_copy(own, ag.at[0], own_sem)

    @pl.when(tp == 0)
    def _():
        own_copy.start()

    for k in range(slots):
        if need(k) < rows:
            for c in range(fine):
                ag[k, META + rows * c + need(k):META + rows * (c + 1), :] = jnp.zeros(
                    (rows - need(k), LANES), BF16
                )

    bi = lax.broadcasted_iota(jnp.int32, (BATCH * rows, BATCH * rows), 0)
    bj = lax.broadcasted_iota(jnp.int32, (BATCH * rows, BATCH * rows), 1)
    upper[...] = jnp.where((bi // rows == bj // rows) & (bi < bj), 1.0, 0.0).astype(BF16)

    @pl.when(tp == 0)
    def _():
        own_copy.wait()

    half_cols = width // 2

    def x_copy(b, h):
        return pltpu.make_async_remote_copy(
            src_ref=x_own.at[b, h], dst_ref=x_sib.at[b, h], send_sem=x_ss.at[b, h],
            recv_sem=x_rs.at[b, h], device_id={"tp": sibling}, device_id_type=MESH,
        )

    def p_copy(b, h):
        return pltpu.make_async_remote_copy(
            src_ref=p_sib.at[b, h], dst_ref=p_rcv.at[b, h], send_sem=p_ss.at[b, h],
            recv_sem=p_rs.at[b, h], device_id={"tp": sibling}, device_id_type=MESH,
        )

    wide = BATCH * rows
    each = BATCH * cap

    def routing(b):
        per_tile = LANES // rows
        lane = lax.broadcasted_iota(jnp.int32, (META, LANES), 1) // rows
        for i in range(wide // LANES):
            mm = ag[b * BATCH + i * per_tile, 0:META, :].astype(F32)
            for j in range(1, per_tile):
                mm = jnp.where(lane == j, ag[b * BATCH + i * per_tile + j, 0:META, :].astype(F32), mm)
            meta_s[:, i * LANES:(i + 1) * LANES] = mm
        ids = [meta_s[k:k + 1, :] for k in range(4)]
        parts = [[meta_s[4 * (p + 1) + k:4 * (p + 1) + k + 1, :] for k in range(4)] for p in range(3)]
        row8 = lax.broadcasted_iota(jnp.int32, (8, wide), 0)
        members, gates = [], []
        for e in range(local):
            eid = (me * local + e).astype(F32)
            hits = [jnp.where(i == eid, 1.0, 0.0) for i in ids]
            members.append(sum(hits))
            gates.append([sum(h * g for h, g in zip(hits, part)) for part in parts])
        stacked = jnp.zeros((8, wide), F32)
        for e in range(local):
            stacked = jnp.where(row8 == e, members[e], stacked)
        rank_s[...] = dot(stacked.astype(BF16), upper[...])
        block = lax.broadcasted_iota(jnp.int32, (1, wide), 1) // rows
        row = lax.broadcasted_iota(jnp.int32, (each, wide), 0)
        for e in range(local):
            rank = rank_s[e:e + 1, :].astype(jnp.int32)
            key = jnp.where(members[e] > 0.5, block * cap + rank, -1)
            pick = jnp.where(row == key, 1.0, 0.0)
            sel[e * each:(e + 1) * each, :] = pick.astype(BF16)
            for p in range(3):
                at = (p * local + e) * each
                gsel[lax.rem(b, 2), at:at + each, :] = (pick * gates[e][p]).astype(BF16)

    def select(b, c):
        block = jnp.concatenate([
            jnp.concatenate(
                [ag[b * BATCH + j, META + rows * at:META + rows * (at + 1), :] for j in range(BATCH)],
                axis=0,
            )
            for at in range(c * (CW // LANES), (c + 1) * (CW // LANES))
        ], axis=1)
        h, at = divmod(c, half_ch)
        x_own[b, h, :, at * CW:(at + 1) * CW] = dot(sel[...], block).astype(BF16)

    def expert_in(b, e, h):
        return jnp.concatenate(
            [x_own[b, h, e * each:(e + 1) * each, :], x_sib[b, h, e * each:(e + 1) * each, :]], axis=0
        )

    def half(h):
        return pl.ds(pl.multiple_of(h * half_cols, half_cols), half_cols)

    def activate(e, gate, up):
        hid[e] = (gate / (1.0 + jnp.exp(-gate)) * up).astype(BF16)

    def gate_up(b, e, h):
        x = expert_in(b, e, h)
        gate = dot(x, wg[e, h * half_cols:(h + 1) * half_cols, :])
        up = dot(x, wu[e, h * half_cols:(h + 1) * half_cols, :])
        if h == 0:
            acc[0], acc[1] = gate, up
        else:
            activate(e, acc[0] + gate, acc[1] + up)

    def down(b, e, h):
        y = dot(hid[e], wd[e, :, h * half_cols:(h + 1) * half_cols]).astype(BF16)
        p_own[b, h, e * each:(e + 1) * each, :] = y[:each]
        p_sib[b, h, e * each:(e + 1) * each, :] = y[each:]

    def combine(b, h, at):
        cols = slice(at * CW, (at + 1) * CW)
        y = (p_own[b, h, :, cols].astype(F32) + p_rcv[b, h, :, cols].astype(F32)).astype(BF16)
        g = tdot(gsel[lax.rem(b, 2)], jnp.concatenate([y, y, y], axis=0))
        for j in range(BATCH):
            contrib[b * BATCH + j, h * half_ch + at] = g[j * rows:(j + 1) * rows]

    def pieces(b):
        call = functools.partial
        work = {0: [call(routing, b)]}
        for c in range(nch):
            work[1 + c] = [call(select, b, c)]
        for h in range(2):
            work[(h + 1) * half_ch].append(lambda h=h: x_copy(b, h).start())
            work[17 + h] = [lambda h=h: x_copy(b, h).wait_recv(), call(gate_up, b, 0, h)]
            work[19 + h] = [call(down, b, 0, h)]
            work[21 + h] = [call(gate_up, b, 1, h)]
            work[23 + h] = [call(down, b, 1, h), lambda h=h: p_copy(b, h).start()]

        def joined(calls):
            def go():
                for each_call in calls:
                    each_call()
            return go

        return {at: joined(calls) for at, calls in work.items()}

    def combine_at(b, i):
        h, at = divmod(i, half_ch)
        if at == 0:
            p_copy(b, h).wait_recv()
        combine(b, h, at)

    def combine_place(b, i):
        if 9 <= i < 9 + nch:
            combine_at(b, i - 9)

    def ag_step(b, j, c, final):
        k = b * BATCH + j

        def both(k, count, ahead_count):
            ag_copy(own, k, c, count).wait_recv()
            ag_copy(ag.at[k], k + 1, c, ahead_count).start()

        if final:
            k = last * BATCH + j
            if k < slots - 2:
                ag_copy(own, k, c, need(k)).wait_recv()
                if k == slots - 3:
                    ag_copy(ag.at[k], k + 2, c, need(k + 2), ahead2).start()
                ag_copy(ag.at[k], k + 1, c, need(k + 1)).start()
            else:
                ag_copy(own, k, c, need(k)).wait_recv()
        elif j == 0:
            pl.when(k + tp >= 1)(lambda: both(k, rows, rows))
        else:
            both(k, rows, rows)

    order = [(j, c) for j in range(BATCH) for c in range(fine)]
    places = 32
    per = len(order) // places

    def window(b, _):
        work = pieces(b - 1)
        for i in range(places):
            for j, c in order[i * per:(i + 1) * per]:
                ag_step(b, j, c, False)
            if i in work:
                pl.when(b > 0)(work[i])
            pl.when(b > 1)(functools.partial(combine_place, b - 2, i))
            if i == 10:
                @pl.when(b == 1)
                def _():
                    for copy in w_copies:
                        copy.wait()
        return 0

    lax.fori_loop(0, last, window, 0)

    work = pieces(last - 1)
    lead = [(j, c) for j, c in order if j < BATCH - 1]
    for i in range(places):
        for j, c in lead[i * len(lead) // places:(i + 1) * len(lead) // places]:
            ag_step(last, j, c, True)
        if i in work:
            work[i]()
        combine_place(last - 2, i)

    for c in range(fine):
        ag_step(last, BATCH - 1, c, True)
        if c == 0:
            routing(last)
        done, odd = divmod(c + 1, CW // LANES)
        if odd == 0:
            select(last, done - 1)
            if done in (half_ch, nch):
                x_copy(last, done // half_ch - 1).start()
    for i in range(half_ch):
        combine_at(last - 1, i)
    partial = {}
    for h in range(2):
        x_copy(last, h).wait_recv()
        for e in range(local):
            x = expert_in(last, e, h)
            for i, w in enumerate((wg, wu)):
                y = dot(x, w[e, h * half_cols:(h + 1) * half_cols, :])
                partial[e, i] = y if h == 0 else partial[e, i] + y
    for e in range(local):
        activate(e, partial[e, 0], partial[e, 1])
    for mine, theirs in ((sibling, tp), (tp, sibling)):
        for e in range(local):
            y = dot(hid[e, each:2 * each, :], wd[e, :, half(theirs)])
            p_sib[last, theirs, e * each:(e + 1) * each, :] = y.astype(BF16)
        p_copy(last, theirs).start()
        for e in range(local):
            y = dot(hid[e, 0:each, :], wd[e, :, half(mine)])
            p_own[last, mine, e * each:(e + 1) * each, :] = y.astype(BF16)

    for i in range(half_ch, nch):
        combine_at(last - 1, i)

    def rs_copy(src, k, at, part):
        span = pl.ds(part[0], part[1] - part[0])
        return pltpu.make_async_remote_copy(
            src_ref=src.at[at, span],
            dst_ref=rs.at[k, at, span],
            send_sem=rs_ss.at[k],
            recv_sem=got.at[k, at * 2 + part[0] // split],
            device_id={"ep": behind},
            device_id_type=MESH,
        )

    def skip_copy(c):
        span = pl.ds(0, need(slots - 1))
        return pltpu.make_async_remote_copy(
            src_ref=rs0.at[c, span],
            dst_ref=skip.at[c],
            send_sem=rs_ss.at[slots - 1],
            recv_sem=got.at[slots + 1, c],
            device_id={"ep": behind2},
            device_id_type=MESH,
        )

    def turn(c):
        at = c + sibling * half_ch
        return jnp.where(at >= nch, at - nch, at)

    for h in (sibling, tp):
        p_copy(last, h).wait_recv()
        for at in range(half_ch):
            combine(last, h, at)
            c = h * half_ch + at
            count = need(slots - 1)
            rs0[c, 0:count, :] = contrib[slots - 1, c, 0:count, :].astype(BF16)
            skip_copy(c).start()
            k, count = slots - 2, need(slots - 2)
            rs[k, c, 0:count, :] = contrib[k, c, 0:count, :].astype(BF16)
            for part in parts(count):
                rs_copy(rs.at[k], k - 1, c, part).start()

    def rs_add(k, to, at, there, count, skipped=0):
        for lo, hi in parts(count):
            mid = max(lo, min(hi, there))
            if lo < mid:
                rs_copy(rs0, k, at, (lo, mid)).wait_recv()
                if lo < skipped:
                    skip_copy(at).wait_recv()
                    contrib[k, at, lo:skipped, :] += skip[at].astype(F32)
                rs[k, at, lo:mid, :] = (
                    rs[k, at, lo:mid, :].astype(F32) + contrib[k, at, lo:mid, :]
                ).astype(BF16)
            if mid < hi:
                rs[k, at, mid:hi, :] = contrib[k, at, mid:hi, :].astype(BF16)
            rs_copy(rs.at[k], to, at, (lo, hi)).start()

    def rs_step(k, there, count, skipped=0):
        for c in range(nch):
            rs_add(k, k - 1, turn(c), there, count, skipped)

    k = slots - 3
    rs_step(k, need(k + 1), need(k), need(slots - 1))
    k -= 1
    while need(k + 1) < rows:
        rs_step(k, need(k + 1), need(k))
        k -= 1
    top_k = k

    def rs_loop(i, _):
        rs_step(top_k - i, rows, rows)
        return 0

    lax.fori_loop(0, top_k, rs_loop, 0)

    @pl.when(tp == 1)
    def _():
        for c in range(nch):
            rs_add(0, slots, turn(c), rows, rows)
    def ag_sent(k, count):
        size = pl.ds(0, META + fine * count)
        pltpu.make_async_remote_copy(
            src_ref=ag.at[k, size], dst_ref=ag.at[k, size], send_sem=ag_ss.at[k],
            recv_sem=got.at[k, 0], device_id={"ep": ahead}, device_id_type=MESH,
        ).wait_send()

    def rs_sent(k, count):
        size = pl.ds(0, count)
        pltpu.make_async_remote_copy(
            src_ref=rs.at[k, :, size], dst_ref=rs.at[k, :, size], send_sem=rs_ss.at[k],
            recv_sem=got.at[k, 0], device_id={"ep": behind}, device_id_type=MESH,
        ).wait_send()

    pl.when(tp == 1)(functools.partial(ag_sent, 0, rows))
    for k in range(1, slots):
        ag_sent(k, need(k))
    for b in range(batches):
        for h in range(2):
            x_copy(b, h).wait_send()
            p_copy(b, h).wait_send()
    for k in range(3, slots - 2):
        rs_sent(k, need(k + 1))

    end = jnp.where(tp == 1, slots, 0)
    share = (1 - tp).astype(F32)

    def f_copy(c):
        return pltpu.make_async_remote_copy(
            src_ref=rs0.at[c], dst_ref=fin.at[c], send_sem=f_ss.at[c],
            recv_sem=f_rs.at[c], device_id={"tp": sibling}, device_id_type=MESH,
        )

    size = pl.ds(0, need(slots - 1))
    pltpu.make_async_remote_copy(
        src_ref=rs0.at[:, size], dst_ref=rs0.at[:, size], send_sem=rs_ss.at[slots - 1],
        recv_sem=got.at[slots - 1, 0], device_id={"ep": behind2}, device_id_type=MESH,
    ).wait_send()
    for c in range(nch):
        at = turn(c)
        for part in parts(rows):
            rs_copy(rs0, end, at, part).wait_recv()
        v = (rs[end, at].astype(F32) + share * contrib[0, at]).astype(BF16)
        y = dot(perm[:, 0:rows], v)
        if c < half_ch:
            rs0[c] = y.astype(BF16)
            f_copy(c).start()
        else:
            i = c - half_ch
            f_copy(i).wait_recv()
            out_ref[:, i * CW:(i + 1) * CW] = (y + fin[i].astype(F32)).astype(BF16)

    for k in range(3):
        rs_sent(k, need(k + 1))

    @pl.when(tp == 1)
    def _():
        rs_sent(slots, rows)

    for c in range(half_ch):
        f_copy(c).wait_send()


def on_device(tokens, norm_gain, groups, picks, gates, w_gate, w_up, w_down):
    rows, width = tokens.shape
    top = picks.shape[1]
    local, _, ffl = w_gate.shape
    n = lax.axis_size("ep")
    group_experts = n * local // GROUPS
    cap = rows * top // group_experts
    slots = n // 2
    batches = slots // BATCH
    nch = width // CW
    batch_rows = local * BATCH * cap
    vmem = pltpu.VMEM
    dma = pltpu.SemaphoreType.DMA
    return pl.pallas_call(
        functools.partial(kernel, n, rows, width, local, cap, group_experts),
        out_shape=pltpu.VMEM((rows, width // 2), BF16),
        in_specs=[pl.BlockSpec(memory_space=pltpu.VMEM)] * 5 + [pl.BlockSpec(memory_space=pl.ANY)] * 3,
        out_specs=pl.BlockSpec(memory_space=pltpu.VMEM),
        scratch_shapes=[
            vmem((META + rows * width // LANES, LANES), BF16),
            vmem((slots, META + rows * width // LANES, LANES), BF16),
            vmem((slots + 1, nch, rows, CW), BF16),
            vmem((nch, rows, CW), BF16),
            vmem((slots, nch, rows, CW), F32),
            vmem(w_gate.shape, BF16),
            vmem(w_up.shape, BF16),
            vmem(w_down.shape, BF16),
            vmem((batches, 2, batch_rows, width // 2), BF16),
            vmem((batches, 2, batch_rows, width // 2), BF16),
            vmem((batches, 2, batch_rows, width // 2), BF16),
            vmem((batches, 2, batch_rows, width // 2), BF16),
            vmem((batches, 2, batch_rows, width // 2), BF16),
            vmem((nch // 2, rows, CW), BF16),
            vmem((batch_rows, BATCH * rows), BF16),
            vmem((2, 3 * batch_rows, BATCH * rows), BF16),
            vmem((META, BATCH * rows), F32),
            vmem((8, BATCH * rows), F32),
            vmem((BATCH * rows, BATCH * rows), BF16),
            vmem((local, 2 * BATCH * cap, ffl), BF16),
            vmem((rows, BATCH * rows), BF16),
            vmem((nch, local * cap, CW), BF16),
            vmem((2, 2 * BATCH * cap, ffl), F32),
            dma((slots,)), dma((slots + 2, width // LANES)), dma((slots + 1,)),
            dma((batches, 2)), dma((batches, 2)), dma((batches, 2)), dma((batches, 2)),
            dma((nch // 2,)), dma((nch // 2,)), dma((3,)), dma,
        ],
        compiler_params=pltpu.CompilerParams(
            collective_id=0, has_side_effects=True, vmem_limit_bytes=60 * 2**20
        ),
    )(
        tokens, norm_gain.reshape(1, width), groups.reshape(1, rows), picks.T, gates.T,
        w_gate, w_up, w_down,
    )


def solution(mesh):
    in_specs = (
        P(("grp", "ep"), None),
        P(),
        P(("grp", "ep")),
        P(("grp", "ep"), None),
        P(("grp", "ep"), None),
        P("ep", None, "tp"),
        P("ep", None, "tp"),
        P("ep", "tp", None),
    )
    out_specs = P(("grp", "ep"), "tp")
    return jax.shard_map(
        on_device, mesh=mesh, in_specs=in_specs, out_specs=out_specs, check_vma=False
    )
```

```python
import functools

import jax
import jax.numpy as jnp
from jax import lax
from jax.experimental import pallas as pl
from jax.experimental.pallas import tpu as pltpu
from jax.sharding import PartitionSpec as P

GROUPS = 2
MESH = pl.DeviceIdType.MESH
F32 = jnp.float32
BF16 = jnp.bfloat16
CW = 256
LANES = 128
META = 16
BATCH = 4

epsilon = 1e-06


def dot(a, b):
    return jnp.dot(a, b, preferred_element_type=F32)


def tdot(a, b):
    return lax.dot_general(a, b, (((0,), (0,)), ((), ())), preferred_element_type=F32)


def kernel(
    n, rows, width, local, cap, group_experts,
    tok_ref, gain_ref, grp_ref, pick_ref, gate_ref, wg_hbm, wu_hbm, wd_hbm, out_ref,
    own, ag, rs, rs0, contrib, wg, wu, wd, x_own, x_sib, p_own, p_sib, p_rcv, fin,
    sel, gsel, meta_s, rank_s, upper, hid, perm, skip, acc,
    ag_ss, got, rs_ss, x_ss, x_rs, p_ss, p_rs, f_ss, f_rs, w_sem, own_sem,
):
    slots = n // 2
    batches = slots // BATCH
    last = batches - 1
    nch = width // CW
    half_ch = nch // 2
    fine = width // LANES
    me = lax.axis_index("ep")
    tp = lax.axis_index("tp")
    right, left = lax.rem(me + 1, n), lax.rem(me + n - 1, n)
    ahead = jnp.where(tp == 1, right, left)
    behind = jnp.where(tp == 1, left, right)
    ahead2 = lax.rem(ahead + ahead - me + n, n)
    behind2 = lax.rem(behind + behind - me + n, n)
    reach = slots - 1 + tp
    sibling = 1 - tp

    barrier = pltpu.get_barrier_semaphore()
    for peer in (ahead2, behind2, ahead, behind):
        pl.semaphore_signal(barrier, inc=1, device_id={"ep": peer}, device_id_type=MESH)
    pl.semaphore_signal(barrier, inc=1, device_id={"tp": sibling}, device_id_type=MESH)

    w_copies = [
        pltpu.make_async_copy(src, dst, w_sem.at[i])
        for i, (src, dst) in enumerate(((wg_hbm, wg), (wu_hbm, wu), (wd_hbm, wd)))
    ]
    for copy in w_copies:
        copy.start()

    split = rows // 2

    def parts(count):
        return [(lo, min(count, lo + split)) for lo in range(0, count, split)]

    def need(k):
        return min(rows, local * cap * (slots - k))

    ri = lax.broadcasted_iota(jnp.int32, (rows, rows), 0)
    ci = lax.broadcasted_iota(jnp.int32, (rows, rows), 1)
    ids = grp_ref[...] * group_experts + pick_ref[...]
    chip = lax.div(ids, jnp.full(ids.shape, local, jnp.int32))
    dist = (chip - me) * (2 * tp - 1) + n
    dist = jnp.where(dist >= n, dist - n, dist)
    dist = jnp.where(dist <= reach, dist, 0).astype(F32)
    far_row = jnp.max(dist, axis=0, keepdims=True)
    far = jnp.sum(jnp.where(ri == ci, far_row, 0.0), axis=1, keepdims=True)
    before = (far_row > far) | ((far_row == far) & (ci < ri))
    place = jnp.sum(jnp.where(before, 1.0, 0.0), axis=1, keepdims=True).astype(jnp.int32)
    lane = lax.rem(
        lax.broadcasted_iota(jnp.int32, (rows, BATCH * rows), 1),
        jnp.full((rows, BATCH * rows), rows, jnp.int32),
    )
    perm[...] = jnp.where(lane == place, 1.0, 0.0).astype(BF16)

    g = gate_ref[...]
    hi = g.astype(BF16).astype(F32)
    mid = (g - hi).astype(BF16).astype(F32)
    low = g - hi - mid
    for i, part in enumerate((ids.astype(F32), hi, mid, low)):
        meta_s[4 * i:4 * (i + 1), 0:LANES] = dot(part.astype(BF16), perm[:, 0:LANES])
    own[0:META, :] = meta_s[:, 0:LANES].astype(BF16)

    total = jnp.zeros((rows, CW), F32)
    for c in range(nch):
        v = tok_ref[:, c * CW:(c + 1) * CW].astype(F32)
        total = total + v * v
    scale = lax.rsqrt(jnp.sum(total, axis=1, keepdims=True) / width + epsilon)

    def ag_copy(src, k, c, count, to=ahead):
        first = 0 if c == 0 else META + rows * c
        span = pl.ds(first, META + rows * c + count - first)
        return pltpu.make_async_remote_copy(
            src_ref=src.at[span],
            dst_ref=ag.at[k, span],
            send_sem=ag_ss.at[k],
            recv_sem=got.at[k, c],
            device_id={"ep": to},
            device_id_type=MESH,
        )

    pl.semaphore_wait(barrier, 5)
    for c in range(nch):
        v = tok_ref[:, c * CW:(c + 1) * CW].astype(F32)
        normed = (v * scale * gain_ref[:, c * CW:(c + 1) * CW]).astype(BF16)
        sorted_rows = tdot(perm[:, 0:rows], normed).astype(BF16)
        for i in range(CW // LANES):
            at = c * (CW // LANES) + i
            own[META + rows * at:META + rows * (at + 1), :] = sorted_rows[:, i * LANES:(i + 1) * LANES]
            ag_copy(own, 1 - tp, at, rows).start()

    own_copy = pltpu.make_async_copy(own, ag.at[0], own_sem)

    @pl.when(tp == 0)
    def _():
        own_copy.start()

    for k in range(slots):
        if need(k) < rows:
            for c in range(fine):
                ag[k, META + rows * c + need(k):META + rows * (c + 1), :] = jnp.zeros(
                    (rows - need(k), LANES), BF16
                )

    bi = lax.broadcasted_iota(jnp.int32, (BATCH * rows, BATCH * rows), 0)
    bj = lax.broadcasted_iota(jnp.int32, (BATCH * rows, BATCH * rows), 1)
    upper[...] = jnp.where((bi // rows == bj // rows) & (bi < bj), 1.0, 0.0).astype(BF16)

    @pl.when(tp == 0)
    def _():
        own_copy.wait()

    half_cols = width // 2

    def x_copy(b, h):
        return pltpu.make_async_remote_copy(
            src_ref=x_own.at[b, h], dst_ref=x_sib.at[b, h], send_sem=x_ss.at[b, h],
            recv_sem=x_rs.at[b, h], device_id={"tp": sibling}, device_id_type=MESH,
        )

    def p_copy(b, h):
        return pltpu.make_async_remote_copy(
            src_ref=p_sib.at[b, h], dst_ref=p_rcv.at[b, h], send_sem=p_ss.at[b, h],
            recv_sem=p_rs.at[b, h], device_id={"tp": sibling}, device_id_type=MESH,
        )

    wide = BATCH * rows
    each = BATCH * cap

    def routing(b):
        per_tile = LANES // rows
        lane = lax.broadcasted_iota(jnp.int32, (META, LANES), 1) // rows
        for i in range(wide // LANES):
            mm = ag[b * BATCH + i * per_tile, 0:META, :].astype(F32)
            for j in range(1, per_tile):
                mm = jnp.where(lane == j, ag[b * BATCH + i * per_tile + j, 0:META, :].astype(F32), mm)
            meta_s[:, i * LANES:(i + 1) * LANES] = mm
        ids = [meta_s[k:k + 1, :] for k in range(4)]
        parts = [[meta_s[4 * (p + 1) + k:4 * (p + 1) + k + 1, :] for k in range(4)] for p in range(3)]
        row8 = lax.broadcasted_iota(jnp.int32, (8, wide), 0)
        members, gates = [], []
        for e in range(local):
            eid = (me * local + e).astype(F32)
            hits = [jnp.where(i == eid, 1.0, 0.0) for i in ids]
            members.append(sum(hits))
            gates.append([sum(h * g for h, g in zip(hits, part)) for part in parts])
        stacked = jnp.zeros((8, wide), F32)
        for e in range(local):
            stacked = jnp.where(row8 == e, members[e], stacked)
        rank_s[...] = dot(stacked.astype(BF16), upper[...])
        block = lax.broadcasted_iota(jnp.int32, (1, wide), 1) // rows
        row = lax.broadcasted_iota(jnp.int32, (each, wide), 0)
        for e in range(local):
            rank = rank_s[e:e + 1, :].astype(jnp.int32)
            key = jnp.where(members[e] > 0.5, block * cap + rank, -1)
            pick = jnp.where(row == key, 1.0, 0.0)
            sel[e * each:(e + 1) * each, :] = pick.astype(BF16)
            for p in range(3):
                at = (p * local + e) * each
                gsel[lax.rem(b, 2), at:at + each, :] = (pick * gates[e][p]).astype(BF16)

    def select(b, c):
        block = jnp.concatenate([
            jnp.concatenate(
                [ag[b * BATCH + j, META + rows * at:META + rows * (at + 1), :] for j in range(BATCH)],
                axis=0,
            )
            for at in range(c * (CW // LANES), (c + 1) * (CW // LANES))
        ], axis=1)
        h, at = divmod(c, half_ch)
        x_own[b, h, :, at * CW:(at + 1) * CW] = dot(sel[...], block).astype(BF16)

    def expert_in(b, e, h):
        return jnp.concatenate(
            [x_own[b, h, e * each:(e + 1) * each, :], x_sib[b, h, e * each:(e + 1) * each, :]], axis=0
        )

    def half(h):
        return pl.ds(pl.multiple_of(h * half_cols, half_cols), half_cols)

    def activate(e, gate, up):
        hid[e] = (gate / (1.0 + jnp.exp(-gate)) * up).astype(BF16)

    def gate_up(b, e, h):
        x = expert_in(b, e, h)
        gate = dot(x, wg[e, h * half_cols:(h + 1) * half_cols, :])
        up = dot(x, wu[e, h * half_cols:(h + 1) * half_cols, :])
        if h == 0:
            acc[0], acc[1] = gate, up
        else:
            activate(e, acc[0] + gate, acc[1] + up)

    def down(b, e, h):
        y = dot(hid[e], wd[e, :, h * half_cols:(h + 1) * half_cols]).astype(BF16)
        p_own[b, h, e * each:(e + 1) * each, :] = y[:each]
        p_sib[b, h, e * each:(e + 1) * each, :] = y[each:]

    def combine(b, h, at):
        cols = slice(at * CW, (at + 1) * CW)
        y = (p_own[b, h, :, cols].astype(F32) + p_rcv[b, h, :, cols].astype(F32)).astype(BF16)
        g = tdot(gsel[lax.rem(b, 2)], jnp.concatenate([y, y, y], axis=0))
        for j in range(BATCH):
            contrib[b * BATCH + j, h * half_ch + at] = g[j * rows:(j + 1) * rows]

    def pieces(b):
        call = functools.partial
        work = {0: [call(routing, b)]}
        for c in range(nch):
            work[1 + c] = [call(select, b, c)]
        for h in range(2):
            work[(h + 1) * half_ch].append(lambda h=h: x_copy(b, h).start())
            work[17 + h] = [lambda h=h: x_copy(b, h).wait_recv(), call(gate_up, b, 0, h)]
            work[19 + h] = [call(down, b, 0, h)]
            work[21 + h] = [call(gate_up, b, 1, h)]
            work[23 + h] = [call(down, b, 1, h), lambda h=h: p_copy(b, h).start()]

        def joined(calls):
            def go():
                for each_call in calls:
                    each_call()
            return go

        return {at: joined(calls) for at, calls in work.items()}

    def combine_at(b, i):
        h, at = divmod(i, half_ch)
        if at == 0:
            p_copy(b, h).wait_recv()
        combine(b, h, at)

    def combine_place(b, i):
        if 9 <= i < 9 + nch:
            combine_at(b, i - 9)

    def ag_step(b, j, c, final):
        k = b * BATCH + j

        def both(k, count, ahead_count):
            ag_copy(own, k, c, count).wait_recv()
            ag_copy(ag.at[k], k + 1, c, ahead_count).start()

        if final:
            k = last * BATCH + j
            if k < slots - 2:
                ag_copy(own, k, c, need(k)).wait_recv()
                if k == slots - 3:
                    ag_copy(ag.at[k], k + 2, c, need(k + 2), ahead2).start()
                ag_copy(ag.at[k], k + 1, c, need(k + 1)).start()
            else:
                ag_copy(own, k, c, need(k)).wait_recv()
        elif j == 0:
            pl.when(k + tp >= 1)(lambda: both(k, rows, rows))
        else:
            both(k, rows, rows)

    order = [(j, c) for j in range(BATCH) for c in range(fine)]
    places = 32
    per = len(order) // places

    def window(b, _):
        work = pieces(b - 1)
        for i in range(places):
            for j, c in order[i * per:(i + 1) * per]:
                ag_step(b, j, c, False)
            if i in work:
                pl.when(b > 0)(work[i])
            pl.when(b > 1)(functools.partial(combine_place, b - 2, i))
            if i == 10:
                @pl.when(b == 1)
                def _():
                    for copy in w_copies:
                        copy.wait()
        return 0

    lax.fori_loop(0, last, window, 0)

    work = pieces(last - 1)
    lead = [(j, c) for j, c in order if j < BATCH - 1]
    for i in range(places):
        for j, c in lead[i * len(lead) // places:(i + 1) * len(lead) // places]:
            ag_step(last, j, c, True)
        if i in work:
            work[i]()
        combine_place(last - 2, i)

    for c in range(fine):
        ag_step(last, BATCH - 1, c, True)
        if c == 0:
            routing(last)
        done, odd = divmod(c + 1, CW // LANES)
        if odd == 0:
            select(last, done - 1)
            if done in (half_ch, nch):
                x_copy(last, done // half_ch - 1).start()
    partial = {}
    for h in range(2):
        x_copy(last, h).wait_recv()
        for e in range(local):
            x = expert_in(last, e, h)
            for i, w in enumerate((wg, wu)):
                y = dot(x, w[e, h * half_cols:(h + 1) * half_cols, :])
                partial[e, i] = y if h == 0 else partial[e, i] + y
    for e in range(local):
        activate(e, partial[e, 0], partial[e, 1])
    for mine, theirs in ((sibling, tp), (tp, sibling)):
        for e in range(local):
            y = dot(hid[e, each:2 * each, :], wd[e, :, half(theirs)])
            p_sib[last, theirs, e * each:(e + 1) * each, :] = y.astype(BF16)
        p_copy(last, theirs).start()
        for e in range(local):
            y = dot(hid[e, 0:each, :], wd[e, :, half(mine)])
            p_own[last, mine, e * each:(e + 1) * each, :] = y.astype(BF16)

    def rs_copy(src, k, at, part):
        span = pl.ds(part[0], part[1] - part[0])
        return pltpu.make_async_remote_copy(
            src_ref=src.at[at, span],
            dst_ref=rs.at[k, at, span],
            send_sem=rs_ss.at[k],
            recv_sem=got.at[k, at * 2 + part[0] // split],
            device_id={"ep": behind},
            device_id_type=MESH,
        )

    def skip_copy(c):
        span = pl.ds(0, need(slots - 1))
        return pltpu.make_async_remote_copy(
            src_ref=rs0.at[c, span],
            dst_ref=skip.at[c],
            send_sem=rs_ss.at[slots - 1],
            recv_sem=got.at[slots + 1, c],
            device_id={"ep": behind2},
            device_id_type=MESH,
        )

    def turn(c):
        at = c + sibling * half_ch
        return jnp.where(at >= nch, at - nch, at)

    for h in (sibling, tp):
        p_copy(last, h).wait_recv()
        for at in range(half_ch):
            combine(last, h, at)
            c = h * half_ch + at
            count = need(slots - 1)
            rs0[c, 0:count, :] = contrib[slots - 1, c, 0:count, :].astype(BF16)
            skip_copy(c).start()
            k, count = slots - 2, need(slots - 2)
            rs[k, c, 0:count, :] = contrib[k, c, 0:count, :].astype(BF16)
            for part in parts(count):
                rs_copy(rs.at[k], k - 1, c, part).start()

    for i in range(nch):
        combine_at(last - 1, i)

    def rs_add(k, to, at, there, count, skipped=0):
        for lo, hi in parts(count):
            mid = max(lo, min(hi, there))
            if lo < mid:
                rs_copy(rs0, k, at, (lo, mid)).wait_recv()
                if lo < skipped:
                    skip_copy(at).wait_recv()
                    contrib[k, at, lo:skipped, :] += skip[at].astype(F32)
                rs[k, at, lo:mid, :] = (
                    rs[k, at, lo:mid, :].astype(F32) + contrib[k, at, lo:mid, :]
                ).astype(BF16)
            if mid < hi:
                rs[k, at, mid:hi, :] = contrib[k, at, mid:hi, :].astype(BF16)
            rs_copy(rs.at[k], to, at, (lo, hi)).start()

    def rs_step(k, there, count, skipped=0):
        for c in range(nch):
            rs_add(k, k - 1, turn(c), there, count, skipped)

    k = slots - 3
    rs_step(k, need(k + 1), need(k), need(slots - 1))
    k -= 1
    while need(k + 1) < rows:
        rs_step(k, need(k + 1), need(k))
        k -= 1
    top_k = k

    def rs_loop(i, _):
        rs_step(top_k - i, rows, rows)
        return 0

    lax.fori_loop(0, top_k, rs_loop, 0)

    @pl.when(tp == 1)
    def _():
        for c in range(nch):
            rs_add(0, slots, turn(c), rows, rows)
    def ag_sent(k, count):
        size = pl.ds(0, META + fine * count)
        pltpu.make_async_remote_copy(
            src_ref=ag.at[k, size], dst_ref=ag.at[k, size], send_sem=ag_ss.at[k],
            recv_sem=got.at[k, 0], device_id={"ep": ahead}, device_id_type=MESH,
        ).wait_send()

    def rs_sent(k, count):
        size = pl.ds(0, count)
        pltpu.make_async_remote_copy(
            src_ref=rs.at[k, :, size], dst_ref=rs.at[k, :, size], send_sem=rs_ss.at[k],
            recv_sem=got.at[k, 0], device_id={"ep": behind}, device_id_type=MESH,
        ).wait_send()

    pl.when(tp == 1)(functools.partial(ag_sent, 0, rows))
    for k in range(1, slots):
        ag_sent(k, need(k))
    for b in range(batches):
        for h in range(2):
            x_copy(b, h).wait_send()
            p_copy(b, h).wait_send()
    for k in range(3, slots - 2):
        rs_sent(k, need(k + 1))

    end = jnp.where(tp == 1, slots, 0)
    share = (1 - tp).astype(F32)

    def f_copy(c):
        return pltpu.make_async_remote_copy(
            src_ref=rs0.at[c], dst_ref=fin.at[c], send_sem=f_ss.at[c],
            recv_sem=f_rs.at[c], device_id={"tp": sibling}, device_id_type=MESH,
        )

    size = pl.ds(0, need(slots - 1))
    pltpu.make_async_remote_copy(
        src_ref=rs0.at[:, size], dst_ref=rs0.at[:, size], send_sem=rs_ss.at[slots - 1],
        recv_sem=got.at[slots - 1, 0], device_id={"ep": behind2}, device_id_type=MESH,
    ).wait_send()
    for c in range(nch):
        at = turn(c)
        for part in parts(rows):
            rs_copy(rs0, end, at, part).wait_recv()
        v = (rs[end, at].astype(F32) + share * contrib[0, at]).astype(BF16)
        y = dot(perm[:, 0:rows], v)
        if c < half_ch:
            rs0[c] = y.astype(BF16)
            f_copy(c).start()
        else:
            i = c - half_ch
            f_copy(i).wait_recv()
            out_ref[:, i * CW:(i + 1) * CW] = (y + fin[i].astype(F32)).astype(BF16)

    for k in range(3):
        rs_sent(k, need(k + 1))

    @pl.when(tp == 1)
    def _():
        rs_sent(slots, rows)

    for c in range(half_ch):
        f_copy(c).wait_send()


def on_device(tokens, norm_gain, groups, picks, gates, w_gate, w_up, w_down):
    rows, width = tokens.shape
    top = picks.shape[1]
    local, _, ffl = w_gate.shape
    n = lax.axis_size("ep")
    group_experts = n * local // GROUPS
    cap = rows * top // group_experts
    slots = n // 2
    batches = slots // BATCH
    nch = width // CW
    batch_rows = local * BATCH * cap
    vmem = pltpu.VMEM
    dma = pltpu.SemaphoreType.DMA
    return pl.pallas_call(
        functools.partial(kernel, n, rows, width, local, cap, group_experts),
        out_shape=pltpu.VMEM((rows, width // 2), BF16),
        in_specs=[pl.BlockSpec(memory_space=pltpu.VMEM)] * 5 + [pl.BlockSpec(memory_space=pl.ANY)] * 3,
        out_specs=pl.BlockSpec(memory_space=pltpu.VMEM),
        scratch_shapes=[
            vmem((META + rows * width // LANES, LANES), BF16),
            vmem((slots, META + rows * width // LANES, LANES), BF16),
            vmem((slots + 1, nch, rows, CW), BF16),
            vmem((nch, rows, CW), BF16),
            vmem((slots, nch, rows, CW), F32),
            vmem(w_gate.shape, BF16),
            vmem(w_up.shape, BF16),
            vmem(w_down.shape, BF16),
            vmem((batches, 2, batch_rows, width // 2), BF16),
            vmem((batches, 2, batch_rows, width // 2), BF16),
            vmem((batches, 2, batch_rows, width // 2), BF16),
            vmem((batches, 2, batch_rows, width // 2), BF16),
            vmem((batches, 2, batch_rows, width // 2), BF16),
            vmem((nch // 2, rows, CW), BF16),
            vmem((batch_rows, BATCH * rows), BF16),
            vmem((2, 3 * batch_rows, BATCH * rows), BF16),
            vmem((META, BATCH * rows), F32),
            vmem((8, BATCH * rows), F32),
            vmem((BATCH * rows, BATCH * rows), BF16),
            vmem((local, 2 * BATCH * cap, ffl), BF16),
            vmem((rows, BATCH * rows), BF16),
            vmem((nch, local * cap, CW), BF16),
            vmem((2, 2 * BATCH * cap, ffl), F32),
            dma((slots,)), dma((slots + 2, width // LANES)), dma((slots + 1,)),
            dma((batches, 2)), dma((batches, 2)), dma((batches, 2)), dma((batches, 2)),
            dma((nch // 2,)), dma((nch // 2,)), dma((3,)), dma,
        ],
        compiler_params=pltpu.CompilerParams(
            collective_id=0, has_side_effects=True, vmem_limit_bytes=60 * 2**20
        ),
    )(
        tokens, norm_gain.reshape(1, width), groups.reshape(1, rows), picks.T, gates.T,
        w_gate, w_up, w_down,
    )


def solution(mesh):
    in_specs = (
        P(("grp", "ep"), None),
        P(),
        P(("grp", "ep")),
        P(("grp", "ep"), None),
        P(("grp", "ep"), None),
        P("ep", None, "tp"),
        P("ep", None, "tp"),
        P("ep", "tp", None),
    )
    out_specs = P(("grp", "ep"), "tp")
    return jax.shard_map(
        on_device, mesh=mesh, in_specs=in_specs, out_specs=out_specs, check_vma=False
    )
```
